128 devices in a mesh: sp: 16 (over z, y), tp: 8 (over x, core).
Axes of the slice: x: 4, y: 4, z: 4, core: 2. Of those that a mesh axis runs over, the one named last changes fastest.
Arguments:
- layer_input: bfloat16 [16, 4096, 2048], P(None, ('sp', 'tp')), may hold values from -6 to 6
- input_gain: float32 [2048], replicated, may hold values from 0.5 to 1.5
- narrowing_matrix: bfloat16 [2048, 512], replicated, may hold values from -0.125 to 0.125
- rotary_down: bfloat16 [2048, 64], replicated, may hold values from -0.125 to 0.125
- summary_scaling: float32 [512], replicated, may hold values from 0.5 to 1.5
- lookup_widening: bfloat16 [512, 16, 128], P('tp'), may hold values from -0.25 to 0.25
- payload_widening: bfloat16 [512, 16, 128], P('tp'), may hold values from -0.25 to 0.25
- query_nope: bfloat16 [16, 16, 128], P('sp', 'tp'), may hold values from -6 to 6
- query_rotary: bfloat16 [16, 16, 64], P('sp', 'tp'), may hold values from -6 to 6
Outputs:
- stored_summaries: bfloat16 [16, 4096, 512], P('sp', None, 'tp')
- rotary_cache: bfloat16 [16, 4096, 64], P('sp', None, 'tp')
- first_read: bfloat16 [16, 16, 128], P('sp', 'tp')
The draws below stay inside these ranges and needn't reach their ends.
All inputs are finite; a program needn't handle non-finite values.
Results may differ from the reference program's by a relative error of at most 0.02.
Values may be sent and summed in bfloat16 or wider, within the bound.
No kernel may reach another device: no remote copies, remote signals or barrier semaphores. Data moves between devices by JAX's collectives and lax.ppermute only.
A program may use at most 64 MiB of HBM per device.

```python
import jax
import jax.numpy as jnp
from jax import lax

BREADTH = 2048
SQUEEZED_SPAN = 512
QK_ROPE = 64
PLAIN_MATCH_SPAN = 128
PAYLOAD_SPAN = 128
READERS = 16
BATCH_ITEMS = 16
SLOTS = 4096


def block_scale(stream_key, dims, shards, least, largest):
    def one(axis_at, blocks):
        heights = jax.random.uniform(jax.random.fold_in(jax.random.fold_in(stream_key, 6), axis_at), (blocks,), jnp.float32, least / len(shards), largest / len(shards))
        return jnp.repeat(jnp.exp(heights), dims[axis_at] // blocks).reshape((-1,) + (1,) * (len(dims) - axis_at - 1))

    factor_of = one(*shards[0])
    for cut in shards[1:]:
        factor_of = factor_of * one(*cut)
    return factor_of


def normal_values(stream_key, extent, deviation, reach, shards=(), held_as=jnp.bfloat16):
    level = block_scale(stream_key, extent, shards, -0.22, 0.18) if shards else 1.0
    entries = jax.random.normal(stream_key, extent, jnp.float32) * deviation * level
    return jnp.minimum(jnp.maximum(entries, -reach), reach).astype(held_as)


def setup_inputs(seed: int = 0) -> dict:
    keys = jax.random.split(jax.random.key(seed), 10)
    layer_input = normal_values(keys[0], (BATCH_ITEMS, SLOTS, BREADTH), 1.0, 6.0, ((1, 128),))
    input_gain = jnp.clip(1.0 + 0.1 * jax.random.normal(keys[1], (BREADTH,), jnp.float32), 0.5, 1.5)
    narrowing_matrix = normal_values(keys[2], (BREADTH, SQUEEZED_SPAN), BREADTH ** -0.5, 0.125)
    rotary_down = normal_values(keys[3], (BREADTH, QK_ROPE), BREADTH ** -0.5, 0.125)
    summary_scaling = jnp.clip(1.0 + 0.1 * jax.random.normal(keys[4], (SQUEEZED_SPAN,), jnp.float32), 0.5, 1.5)
    lookup_widening = normal_values(keys[5], (SQUEEZED_SPAN, READERS, PLAIN_MATCH_SPAN), SQUEEZED_SPAN ** -0.5, 0.25, ((0, 8),))
    payload_widening = normal_values(keys[6], (SQUEEZED_SPAN, READERS, PAYLOAD_SPAN), SQUEEZED_SPAN ** -0.5, 0.25, ((0, 8),))
    query_nope = normal_values(keys[7], (BATCH_ITEMS, READERS, PLAIN_MATCH_SPAN), 1.0, 6.0, ((0, 16), (1, 8)))
    query_rotary = normal_values(keys[8], (BATCH_ITEMS, READERS, QK_ROPE), 1.0, 6.0, ((0, 16), (1, 8)))
    return {"layer_input": layer_input, "input_gain": input_gain, "narrowing_matrix": narrowing_matrix, "rotary_down": rotary_down, "summary_scaling": summary_scaling, "lookup_widening": lookup_widening, "payload_widening": payload_widening, "query_nope": query_nope, "query_rotary": query_rotary}


norm_eps = 1e-06
rotary_base = 10000.0

def rescaled_lines(vector):
    return vector * lax.rsqrt(lax.optimization_barrier(jnp.mean(vector * vector, axis=-1, keepdims=True)) + norm_eps)

def rotate(vector, position):
    half_width = vector.shape[-1] // 2
    frequency = 1.0 / rotary_base ** (jnp.arange(half_width, dtype=jnp.float32) * 2.0 / vector.shape[-1])
    angles = position * frequency
    first_half = vector[..., :half_width]
    second_half = vector[..., half_width:]
    return jnp.concatenate([first_half * jnp.cos(angles) - second_half * jnp.sin(angles), second_half * jnp.cos(angles) + first_half * jnp.sin(angles)], axis=-1)

def reference(layer_input, input_gain, narrowing_matrix, rotary_down, summary_scaling, lookup_widening, payload_widening, query_nope, query_rotary):
    normed = (rescaled_lines(layer_input.astype(jnp.float32)) * input_gain).astype(jnp.bfloat16)
    flat_rows = normed.reshape(BATCH_ITEMS * SLOTS, BREADTH)
    hidden_summary = jnp.dot(flat_rows, narrowing_matrix, preferred_element_type=jnp.float32).astype(jnp.bfloat16)
    rotary = jnp.dot(flat_rows, rotary_down, preferred_element_type=jnp.float32).astype(jnp.bfloat16)
    stored_summaries = (rescaled_lines(hidden_summary.astype(jnp.float32)) * summary_scaling).astype(jnp.bfloat16).reshape(BATCH_ITEMS, SLOTS, SQUEEZED_SPAN)
    positions = jnp.arange(SLOTS, dtype=jnp.float32)[None, :, None]
    rotary_cache = rotate(rotary.astype(jnp.float32).reshape(BATCH_ITEMS, SLOTS, QK_ROPE), positions).astype(jnp.bfloat16)
    absorbed = jnp.einsum('shd,chd->shc', query_nope.astype(jnp.float32), lookup_widening.astype(jnp.float32)).astype(jnp.bfloat16)
    query_turned = rotate(query_rotary.astype(jnp.float32), jnp.float32(SLOTS)).astype(jnp.bfloat16)
    score_scale = (PLAIN_MATCH_SPAN + QK_ROPE) ** (-0.5)
    scores = (jnp.einsum('shc,spc->shp', absorbed.astype(jnp.float32), stored_summaries.astype(jnp.float32)) + jnp.einsum('shr,spr->shp', query_turned.astype(jnp.float32), rotary_cache.astype(jnp.float32))) * score_scale
    attention = jax.nn.softmax(scores, axis=-1).astype(jnp.bfloat16)
    context = jnp.einsum('shp,spc->shc', attention.astype(jnp.float32), stored_summaries.astype(jnp.float32)).astype(jnp.bfloat16)
    values = jnp.einsum('shc,chv->shv', context.astype(jnp.float32), payload_widening.astype(jnp.float32))
    first_read = rescaled_lines(values).astype(jnp.bfloat16)
    return (stored_summaries, rotary_cache, first_read)
```

```python
import jax
import jax.numpy as jnp
from jax import lax
from jax.experimental import pallas as pl
from jax.experimental.pallas import tpu as pltpu
from jax.sharding import Mesh
from jax.sharding import PartitionSpec as P

QK_ROPE = 64
PLAIN_MATCH_SPAN = 128
TP = ("x", "c")
SP_TP = ("sp", "x", "c")

norm_eps = 1e-06
rotary_base = 10000.0
F32 = jnp.float32
BF16 = jnp.bfloat16
LAST = (((1,), (1,)), ((), ()))


def frequencies():
    half = QK_ROPE // 2
    return 1.0 / rotary_base ** (jnp.arange(half, dtype=F32) * 2.0 / QK_ROPE)


def rotate(vector, position):
    half_width = vector.shape[-1] // 2
    angles = position * frequencies()
    first_half = vector[..., :half_width]
    second_half = vector[..., half_width:]
    return jnp.concatenate(
        [
            first_half * jnp.cos(angles) - second_half * jnp.sin(angles),
            second_half * jnp.cos(angles) + first_half * jnp.sin(angles),
        ],
        axis=-1,
    )


def pack_weights_kernel(pay_ref, qn_ref, qr_ref, out_ref):
    pay = pay_ref[...].astype(F32)
    count = out_ref.shape[0]
    for t in range(count):
        for h in range(2):
            out_ref[t, 0:64, h * 128 : (h + 1) * 128] = pay[:, 2 * t + h, :].astype(BF16)
    qn = qn_ref[...].astype(F32)
    qr = qr_ref[...].astype(F32)
    row0 = jnp.concatenate([qn[0:1], qn[1:2]], axis=1)
    row1 = jnp.concatenate([qr[0:1], qr[1:2], jnp.zeros((1, 128), F32)], axis=1)
    block = jnp.concatenate([row0, row1, jnp.zeros((14, 256), F32)], axis=0).astype(BF16)
    for t in range(count):
        out_ref[t, 64:80, :] = block


def project_kernel(x_ref, gain_ref, w_ref, r_ref, scal_ref, cs_ref, out_ref):
    rows = x_ref.shape[0]
    step = 128
    gain = gain_ref[...]
    scal = scal_ref[...]
    seqs = step // 32
    cos = jnp.concatenate([cs_ref[0]] * seqs, axis=0)
    sin = jnp.concatenate([cs_ref[1]] * seqs, axis=0)
    for i in range(rows // step):
        x = x_ref[i * step : (i + 1) * step, :].astype(F32)
        mean = jnp.mean(x * x, axis=-1, keepdims=True)
        normed = (x * lax.rsqrt(mean + norm_eps) * gain).astype(BF16)
        lat = jnp.dot(normed, w_ref[...], preferred_element_type=F32).astype(BF16).astype(F32)
        rot = lax.dot_general(normed, r_ref[...], LAST, preferred_element_type=F32)
        rot = rot.astype(BF16).astype(F32)
        mean = jnp.mean(lat * lat, axis=-1, keepdims=True)
        lat = (lat * lax.rsqrt(mean + norm_eps) * scal).astype(BF16)
        swapped = jnp.concatenate([rot[:, 32:], rot[:, :32]], axis=1)
        rot = rot * cos + swapped * sin
        rot = jnp.concatenate([rot, jnp.zeros_like(rot)], axis=1).astype(BF16)
        for s in range(seqs):
            out_ref[i * seqs + s, :, 0:512] = lat[s * 32 : (s + 1) * 32]
            out_ref[i * seqs + s, :, 512:640] = rot[s * 32 : (s + 1) * 32]


def attend_kernel(z_ref, a0_ref, a1_ref, a2_ref, a3_ref, t_ref, out_ref):
    n = z_ref.shape[0] * z_ref.shape[1]
    lat = z_ref[:, :, 0:512].reshape(n, 512)
    rot = z_ref[:, :, 512:640].reshape(n, 128)
    absorbed = (a0_ref[...] + a1_ref[...]) + (a2_ref[...] + a3_ref[...])
    scores = lax.dot_general(absorbed, lat, LAST, preferred_element_type=F32)
    scores = scores + lax.dot_general(t_ref[...], rot, LAST, preferred_element_type=F32)
    scores = scores * ((PLAIN_MATCH_SPAN + QK_ROPE) ** (-0.5))
    top = jnp.max(scores, axis=-1, keepdims=True).astype(BF16).astype(F32)
    weight = jnp.exp(scores - top)
    total = jnp.sum(weight, axis=-1, keepdims=True)
    context = jnp.dot(weight.astype(BF16), lat, preferred_element_type=F32)
    high = total.astype(BF16).astype(F32)
    low = total - high
    top = jnp.broadcast_to(top, context.shape)
    high = jnp.broadcast_to(high, context.shape)
    low = jnp.broadcast_to(low, context.shape)
    lat_t = lat.T
    rot_t = rot.astype(F32).T
    for t in range(out_ref.shape[0]):
        out_ref[t, 0:64, :] = lat_t[64 * t : 64 * (t + 1)]
        mine = slice(2 * t, 2 * t + 2)
        block = jnp.concatenate(
            [rot_t[8 * t : 8 * t + 8], context[mine], top[mine], high[mine], low[mine]], axis=0
        )
        out_ref[t, 64:80, :] = block.astype(BF16)


def finish_kernel(y_ref, w_ref, st_ref, rt_ref, fr_ref):
    count = y_ref.shape[0]
    for q in range(4):
        for o in range(4):
            for j in range(2):
                lanes = slice((4 * q + o) * 32, (4 * q + o) * 32 + 32)
                tile = jnp.concatenate(
                    [y_ref[4 * j + k, 0:80, lanes] for k in range(4)], axis=1
                )
                at = (4 * q + o) * 256 + j * 128
                st_ref[:, at : at + 128] = tile[0:64]
                rt_ref[:, at : at + 128] = tile[64:72]
    tails = [y_ref[t, 64:80, :].astype(F32)[8:16] for t in range(count)]
    tops = [v[2:4] for v in tails]
    peak = tops[0]
    for v in tops[1:]:
        peak = jnp.maximum(peak, v)
    number = jnp.zeros_like(peak)
    denominator = jnp.zeros_like(peak)
    for v, top in zip(tails, tops):
        scale = jnp.exp(top - peak)
        number = number + scale * v[0:2]
        denominator = denominator + scale * (v[4:6] + v[6:8])
    context = (number / denominator).astype(BF16)
    weight = w_ref[:, 0:64, :].reshape(count * 64, 256)
    values = jnp.dot(context, weight, preferred_element_type=F32)
    values = jnp.concatenate([values[0:1, 0:128], values[1:2, 128:256]], axis=0)
    mean = jnp.mean(values * values, axis=-1, keepdims=True)
    fr_ref[...] = (values * lax.rsqrt(mean + norm_eps)).astype(BF16)


def call(kernel, out_shape, flops, moved):
    return pl.pallas_call(
        kernel,
        out_shape=out_shape,
        cost_estimate=pl.CostEstimate(flops=flops, bytes_accessed=moved, transcendentals=0),
        compiler_params=pltpu.CompilerParams(vmem_limit_bytes=32 * 1024 * 1024),
    )


def shards(
    layer_input,
    input_gain,
    narrowing_matrix,
    rotary_down,
    summary_scaling,
    lookup_widening,
    payload_widening,
    query_nope,
    query_rotary,
):
    seqs, pos_local, width = layer_input.shape
    tp = lax.axis_size(TP)
    sp = lax.axis_size("sp")
    me = lax.axis_index(TP)
    block = lax.axis_index(SP_TP)
    shape = jax.ShapeDtypeStruct

    packed = call(pack_weights_kernel, shape((tp, 80, 256), BF16), 0, 600_000)(
        payload_widening, query_nope[0], query_rotary[0]
    )
    spread = lax.all_to_all(packed, TP, 0, 0, tiled=True)

    positions = (block * pos_local + jnp.arange(pos_local, dtype=jnp.int32)).astype(F32)
    angles = positions[:, None] * frequencies()[None, :]
    cos, sin = jnp.cos(angles), jnp.sin(angles)
    table = jnp.stack(
        [jnp.concatenate([cos, cos], axis=1), jnp.concatenate([-sin, sin], axis=1)]
    )
    sent = call(project_kernel, shape((seqs, pos_local, 640), BF16), 1_300_000_000, 5_000_000)(
        layer_input.reshape(seqs * pos_local, width),
        input_gain[None],
        narrowing_matrix,
        rotary_down.T,
        summary_scaling[None],
        table,
    )
    held = lax.all_to_all(sent, "sp", 0, 0, tiled=True)

    query = spread[:, 64, :].reshape(2 * tp, 128)
    turn = spread[:, 65, 0:128].reshape(2 * tp, QK_ROPE)
    share = jnp.einsum("hd,chd->hc", query, lookup_widening, preferred_element_type=F32)
    share = share.astype(BF16)
    lane = lax.broadcasted_iota(jnp.int32, (2 * tp, 512), 1) // 64
    placed = jnp.where(lane == me, jnp.concatenate([share] * tp, axis=1), jnp.zeros((), BF16))
    other = lax.ppermute(placed, "c", [(0, 1), (1, 0)])
    pair = placed + other
    around = [
        lax.ppermute(pair, "x", [(i, (i + d) % 4) for i in range(4)]) for d in (1, 3, 2)
    ]
    turned = rotate(turn.astype(F32), F32(seqs * 0 + sp * tp * pos_local)).astype(BF16)
    turned = jnp.concatenate([turned, jnp.zeros_like(turned)], axis=1)

    piece = call(attend_kernel, shape((tp, 80, 512), BF16), 600_000_000, 1_300_000)(
        held, pair, *around, turned
    )
    arrived = lax.all_to_all(piece, TP, 0, 0, tiled=True)

    total = sp * tp * pos_local
    stored, rotary, first = call(
        finish_kernel,
        (shape((64, total), BF16), shape((8, total), BF16), shape((2, 128), BF16)),
        10_000_000,
        1_800_000,
    )(arrived, spread)
    return stored.T[None], rotary.T[None], first[None]


def solution(mesh):
    torus = Mesh(mesh.devices.reshape(mesh.shape["sp"], 4, 2), SP_TP)
    in_specs = (
        P(None, SP_TP, None),
        P(),
        P(),
        P(),
        P(),
        P(TP, None, None),
        P(TP, None, None),
        P("sp", TP, None),
        P("sp", TP, None),
    )
    out_specs = (P("sp", None, TP), P("sp", None, TP), P("sp", TP, None))
    return jax.shard_map(
        shards, mesh=torus, in_specs=in_specs, out_specs=out_specs, check_vma=False
    )
```

```python
import jax
import jax.numpy as jnp
from jax import lax
from jax.experimental import pallas as pl
from jax.experimental.pallas import tpu as pltpu
from jax.sharding import Mesh
from jax.sharding import PartitionSpec as P

QK_ROPE = 64
PLAIN_MATCH_SPAN = 128
TP = ("x", "c")
SP_TP = ("sp", "x", "c")

norm_eps = 1e-06
rotary_base = 10000.0
F32 = jnp.float32
BF16 = jnp.bfloat16
LAST = (((1,), (1,)), ((), ()))


def frequencies():
    half = QK_ROPE // 2
    return 1.0 / rotary_base ** (jnp.arange(half, dtype=F32) * 2.0 / QK_ROPE)


def rotate(vector, position):
    half_width = vector.shape[-1] // 2
    angles = position * frequencies()
    first_half = vector[..., :half_width]
    second_half = vector[..., half_width:]
    return jnp.concatenate(
        [
            first_half * jnp.cos(angles) - second_half * jnp.sin(angles),
            second_half * jnp.cos(angles) + first_half * jnp.sin(angles),
        ],
        axis=-1,
    )


def pack_weights_kernel(pay_hbm, qn_hbm, qr_hbm, out_ref, pay_ref, qn_ref, qr_ref, sems):
    copies = [
        pltpu.make_async_copy(pay_hbm, pay_ref, sems.at[0]),
        pltpu.make_async_copy(qn_hbm, qn_ref, sems.at[1]),
        pltpu.make_async_copy(qr_hbm, qr_ref, sems.at[2]),
    ]
    for copy in copies:
        copy.start()
    for copy in copies:
        copy.wait()
    pay = pay_ref[...].astype(F32)
    count = out_ref.shape[0]
    for t in range(count):
        for h in range(2):
            out_ref[t, 0:64, h * 128 : (h + 1) * 128] = pay[:, 2 * t + h, :].astype(BF16)
    qn = qn_ref[...].astype(F32)
    qr = qr_ref[...].astype(F32)
    row0 = jnp.concatenate([qn[0:1], qn[1:2]], axis=1)
    row1 = jnp.concatenate([qr[0:1], qr[1:2], jnp.zeros((1, 128), F32)], axis=1)
    block = jnp.concatenate([row0, row1, jnp.zeros((14, 256), F32)], axis=0).astype(BF16)
    for t in range(count):
        out_ref[t, 64:80, :] = block


def project_kernel(x_hbm, gain_ref, w_ref, r_ref, scal_ref, cs_ref, out_ref, x_ref, sems):
    rows = x_ref.shape[0]
    step = 128
    copies = []
    for i in range(rows // step):
        part = pl.ds(i * step, step)
        copies.append(pltpu.make_async_copy(x_hbm.at[part], x_ref.at[part], sems.at[i]))
        copies[-1].start()
    gain = gain_ref[...]
    scal = scal_ref[...]
    seqs = step // 32
    cos = jnp.concatenate([cs_ref[0]] * seqs, axis=0)
    sin = jnp.concatenate([cs_ref[1]] * seqs, axis=0)
    for i in range(rows // step):
        copies[i].wait()
        x = x_ref[i * step : (i + 1) * step, :].astype(F32)
        mean = jnp.mean(x * x, axis=-1, keepdims=True)
        normed = (x * lax.rsqrt(mean + norm_eps) * gain).astype(BF16)
        lat = jnp.dot(normed, w_ref[...], preferred_element_type=F32).astype(BF16).astype(F32)
        rot = lax.dot_general(normed, r_ref[...], LAST, preferred_element_type=F32)
        rot = rot.astype(BF16).astype(F32)
        mean = jnp.mean(lat * lat, axis=-1, keepdims=True)
        lat = (lat * lax.rsqrt(mean + norm_eps) * scal).astype(BF16)
        swapped = jnp.concatenate([rot[:, 32:], rot[:, :32]], axis=1)
        rot = rot * cos + swapped * sin
        rot = jnp.concatenate([rot, jnp.zeros_like(rot)], axis=1).astype(BF16)
        for s in range(seqs):
            out_ref[i * seqs + s, :, 0:512] = lat[s * 32 : (s + 1) * 32]
            out_ref[i * seqs + s, :, 512:640] = rot[s * 32 : (s + 1) * 32]


def attend_kernel(z_ref, a0_ref, a1_ref, t_ref, out_ref):
    n = z_ref.shape[0] * z_ref.shape[1]
    lat = z_ref[:, :, 0:512].reshape(n, 512)
    rot = z_ref[:, :, 512:640].reshape(n, 128)
    absorbed = a0_ref[...] + a1_ref[...]
    scores = lax.dot_general(absorbed, lat, LAST, preferred_element_type=F32)
    scores = scores + lax.dot_general(t_ref[...], rot, LAST, preferred_element_type=F32)
    scores = scores * ((PLAIN_MATCH_SPAN + QK_ROPE) ** (-0.5))
    top = jnp.max(scores, axis=-1, keepdims=True).astype(BF16).astype(F32)
    weight = jnp.exp(scores - top)
    total = jnp.sum(weight, axis=-1, keepdims=True)
    context = jnp.dot(weight.astype(BF16), lat, preferred_element_type=F32)
    high = total.astype(BF16).astype(F32)
    low = total - high
    top = jnp.broadcast_to(top, context.shape)
    high = jnp.broadcast_to(high, context.shape)
    low = jnp.broadcast_to(low, context.shape)
    lat_t = lat.T
    rot_t = rot.astype(F32).T
    for t in range(out_ref.shape[0]):
        out_ref[t, 0:64, :] = lat_t[64 * t : 64 * (t + 1)]
        mine = slice(2 * t, 2 * t + 2)
        block = jnp.concatenate(
            [rot_t[8 * t : 8 * t + 8], context[mine], top[mine], high[mine], low[mine]], axis=0
        )
        out_ref[t, 64:80, :] = block.astype(BF16)


def finish_kernel(y_ref, w_ref, st_ref, rt_ref, fr_ref):
    count = y_ref.shape[0]
    for q in range(4):
        for o in range(4):
            for j in range(2):
                lanes = slice((4 * q + o) * 32, (4 * q + o) * 32 + 32)
                tile = jnp.concatenate(
                    [y_ref[4 * j + k, 0:80, lanes] for k in range(4)], axis=1
                )
                at = (4 * q + o) * 256 + j * 128
                st_ref[:, at : at + 128] = tile[0:64]
                rt_ref[:, at : at + 128] = tile[64:72]
    tails = [y_ref[t, 64:80, :].astype(F32)[8:16] for t in range(count)]
    tops = [v[2:4] for v in tails]
    peak = tops[0]
    for v in tops[1:]:
        peak = jnp.maximum(peak, v)
    number = jnp.zeros_like(peak)
    denominator = jnp.zeros_like(peak)
    for v, top in zip(tails, tops):
        scale = jnp.exp(top - peak)
        number = number + scale * v[0:2]
        denominator = denominator + scale * (v[4:6] + v[6:8])
    context = (number / denominator).astype(BF16)
    weight = w_ref[:, 0:64, :].reshape(count * 64, 256)
    values = jnp.dot(context, weight, preferred_element_type=F32)
    values = jnp.concatenate([values[0:1, 0:128], values[1:2, 128:256]], axis=0)
    mean = jnp.mean(values * values, axis=-1, keepdims=True)
    fr_ref[...] = (values * lax.rsqrt(mean + norm_eps)).astype(BF16)


def in_hbm(array):
    return pltpu.with_memory_space_constraint(array, pltpu.HBM)


def call(kernel, out_shape, flops, moved, **kwargs):
    return pl.pallas_call(
        kernel,
        out_shape=out_shape,
        **kwargs,
        cost_estimate=pl.CostEstimate(flops=flops, bytes_accessed=moved, transcendentals=0),
        compiler_params=pltpu.CompilerParams(vmem_limit_bytes=32 * 1024 * 1024),
    )


def shards(
    layer_input,
    input_gain,
    narrowing_matrix,
    rotary_down,
    summary_scaling,
    lookup_widening,
    payload_widening,
    query_nope,
    query_rotary,
):
    seqs, pos_local, width = layer_input.shape
    tp = lax.axis_size(TP)
    sp = lax.axis_size("sp")
    me = lax.axis_index(TP)
    block = lax.axis_index(SP_TP)
    shape = jax.ShapeDtypeStruct

    packed = call(
        pack_weights_kernel,
        shape((tp, 80, 256), BF16),
        30_000_000_000,
        60_000_000,
        in_specs=[pl.BlockSpec(memory_space=pltpu.HBM)] * 3,
        scratch_shapes=[
            pltpu.VMEM(payload_widening.shape, BF16),
            pltpu.VMEM(query_nope.shape[1:], BF16),
            pltpu.VMEM(query_rotary.shape[1:], BF16),
            pltpu.SemaphoreType.DMA((3,)),
        ],
    )(in_hbm(payload_widening), in_hbm(query_nope[0]), in_hbm(query_rotary[0]))
    spread = lax.all_to_all(packed, TP, 0, 0, tiled=True)

    positions = (block * pos_local + jnp.arange(pos_local, dtype=jnp.int32)).astype(F32)
    angles = positions[:, None] * frequencies()[None, :]
    cos, sin = jnp.cos(angles), jnp.sin(angles)
    table = jnp.stack(
        [jnp.concatenate([cos, cos], axis=1), jnp.concatenate([-sin, sin], axis=1)]
    )
    whole = pl.BlockSpec(memory_space=pltpu.VMEM)
    sent = call(
        project_kernel,
        shape((seqs, pos_local, 640), BF16),
        1_300_000_000,
        5_000_000,
        in_specs=[pl.BlockSpec(memory_space=pltpu.HBM)] + [whole] * 5,
        scratch_shapes=[
            pltpu.VMEM((seqs * pos_local, width), BF16),
            pltpu.SemaphoreType.DMA((4,)),
        ],
    )(
        in_hbm(layer_input.reshape(seqs * pos_local, width)),
        input_gain[None],
        narrowing_matrix,
        rotary_down.T,
        summary_scaling[None],
        table,
    )
    held = lax.all_to_all(sent, "sp", 0, 0, tiled=True)

    query = spread[:, 64, :].reshape(2 * tp, 128)
    turn = spread[:, 65, 0:128].reshape(2 * tp, QK_ROPE)
    share = jnp.einsum("hd,chd->hc", query, lookup_widening, preferred_element_type=F32)
    share = share.astype(BF16)
    lane = lax.broadcasted_iota(jnp.int32, (2 * tp, 512), 1) // 64
    placed = jnp.where(lane == me, jnp.concatenate([share] * tp, axis=1), jnp.zeros((), BF16))
    placed = placed + lax.ppermute(placed, "c", [(0, 1), (1, 0)])
    placed = placed + lax.ppermute(placed, "x", [(0, 1), (1, 0), (2, 3), (3, 2)])
    other = lax.ppermute(placed, "x", [(0, 3), (3, 0), (1, 2), (2, 1)])
    turned = rotate(turn.astype(F32), F32(seqs * 0 + sp * tp * pos_local)).astype(BF16)
    turned = jnp.concatenate([turned, jnp.zeros_like(turned)], axis=1)

    piece = call(attend_kernel, shape((tp, 80, 512), BF16), 600_000_000, 1_300_000)(
        held, placed, other, turned
    )
    arrived = lax.all_to_all(piece, TP, 0, 0, tiled=True)

    total = sp * tp * pos_local
    stored, rotary, first = call(
        finish_kernel,
        (shape((64, total), BF16), shape((8, total), BF16), shape((2, 128), BF16)),
        10_000_000,
        1_800_000,
    )(arrived, spread)
    return stored.T[None], rotary.T[None], first[None]


def solution(mesh):
    torus = Mesh(mesh.devices.reshape(mesh.shape["sp"], 4, 2), SP_TP)
    in_specs = (
        P(None, SP_TP, None),
        P(),
        P(),
        P(),
        P(),
        P(TP, None, None),
        P(TP, None, None),
        P("sp", TP, None),
        P("sp", TP, None),
    )
    out_specs = (P("sp", None, TP), P("sp", None, TP), P("sp", TP, None))
    return jax.shard_map(
        shards, mesh=torus, in_specs=in_specs, out_specs=out_specs, check_vma=False
    )
```

```python
import jax
import jax.numpy as jnp
from jax import lax
from jax.experimental import pallas as pl
from jax.experimental.pallas import tpu as pltpu
from jax.sharding import Mesh
from jax.sharding import PartitionSpec as P

QK_ROPE = 64
PLAIN_MATCH_SPAN = 128
TP = ("x", "c")
SP_TP = ("sp", "x", "c")

norm_eps = 1e-06
rotary_base = 10000.0
F32 = jnp.float32
BF16 = jnp.bfloat16
FIRST_ROWS = 128
LAST = (((1,), (1,)), ((), ()))


def frequencies():
    half = QK_ROPE // 2
    return 1.0 / rotary_base ** (jnp.arange(half, dtype=F32) * 2.0 / QK_ROPE)


def rotate(vector, position):
    half_width = vector.shape[-1] // 2
    angles = position * frequencies()
    first_half = vector[..., :half_width]
    second_half = vector[..., half_width:]
    return jnp.concatenate(
        [
            first_half * jnp.cos(angles) - second_half * jnp.sin(angles),
            second_half * jnp.cos(angles) + first_half * jnp.sin(angles),
        ],
        axis=-1,
    )


def pack_weights_kernel(
    pay_hbm, qn_hbm, qr_hbm, x_hbm, out_ref, x_ref, pay_ref, qn_ref, qr_ref, sems
):
    fetch = pltpu.make_async_copy(x_hbm.at[pl.ds(0, x_ref.shape[0])], x_ref, sems.at[3])
    copies = [
        pltpu.make_async_copy(pay_hbm, pay_ref, sems.at[0]),
        pltpu.make_async_copy(qn_hbm, qn_ref, sems.at[1]),
        pltpu.make_async_copy(qr_hbm, qr_ref, sems.at[2]),
    ]
    for copy in copies:
        copy.start()
    fetch.start()
    for copy in copies:
        copy.wait()
    pay = pay_ref[...].astype(F32)
    count = out_ref.shape[0]
    for t in range(count):
        for h in range(2):
            out_ref[count - 1 - t, 0:64, h * 128 : (h + 1) * 128] = pay[:, 2 * t + h, :].astype(BF16)
    qn = qn_ref[...].astype(F32)
    qr = qr_ref[...].astype(F32)
    row0 = jnp.concatenate([qn[0:1], qn[1:2]], axis=1)
    row1 = jnp.concatenate([qr[0:1], qr[1:2], jnp.zeros((1, 128), F32)], axis=1)
    block = jnp.concatenate([row0, row1, jnp.zeros((14, 256), F32)], axis=0).astype(BF16)
    for t in range(count):
        out_ref[t, 64:80, :] = block
    fetch.wait()


def project_kernel(
    first_ref, x_hbm, gain_ref, w_ref, r_ref, scal_ref, cs_ref, out_ref, rest_ref, sem
):
    early = first_ref.shape[0]
    rows = early + rest_ref.shape[0]
    step = 128
    fetch = pltpu.make_async_copy(x_hbm.at[pl.ds(early, rows - early)], rest_ref, sem)
    fetch.start()
    gain = gain_ref[...]
    scal = scal_ref[...]
    seqs = step // 32
    cos = jnp.concatenate([cs_ref[0]] * seqs, axis=0)
    sin = jnp.concatenate([cs_ref[1]] * seqs, axis=0)
    for i in range(rows // step):
        at = i * step
        if at == early:
            fetch.wait()
        x = first_ref[at : at + step] if at < early else rest_ref[at - early : at - early + step]
        x = x.astype(F32)
        mean = jnp.mean(x * x, axis=-1, keepdims=True)
        normed = (x * lax.rsqrt(mean + norm_eps) * gain).astype(BF16)
        lat = jnp.dot(normed, w_ref[...], preferred_element_type=F32).astype(BF16).astype(F32)
        rot = lax.dot_general(normed, r_ref[...], LAST, preferred_element_type=F32)
        rot = rot.astype(BF16).astype(F32)
        mean = jnp.mean(lat * lat, axis=-1, keepdims=True)
        lat = (lat * lax.rsqrt(mean + norm_eps) * scal).astype(BF16)
        swapped = jnp.concatenate([rot[:, 32:], rot[:, :32]], axis=1)
        rot = rot * cos + swapped * sin
        rot = jnp.concatenate([rot, jnp.zeros_like(rot)], axis=1).astype(BF16)
        for s in range(seqs):
            slot = out_ref.shape[0] - 1 - (i * seqs + s)
            out_ref[slot, :, 0:512] = lat[s * 32 : (s + 1) * 32]
            out_ref[slot, :, 512:640] = rot[s * 32 : (s + 1) * 32]


def attend_kernel(z_ref, a0_ref, a1_ref, t_ref, out_ref):
    order = range(z_ref.shape[0] - 1, -1, -1)
    lat = jnp.concatenate([z_ref[i, :, 0:512] for i in order], axis=0)
    rot = jnp.concatenate([z_ref[i, :, 512:640] for i in order], axis=0)
    absorbed = a0_ref[...] + a1_ref[...]
    scores = lax.dot_general(absorbed, lat, LAST, preferred_element_type=F32)
    scores = scores + lax.dot_general(t_ref[...], rot, LAST, preferred_element_type=F32)
    scores = scores * ((PLAIN_MATCH_SPAN + QK_ROPE) ** (-0.5))
    top = jnp.max(scores, axis=-1, keepdims=True).astype(BF16).astype(F32)
    weight = jnp.exp(scores - top)
    total = jnp.sum(weight, axis=-1, keepdims=True)
    context = jnp.dot(weight.astype(BF16), lat, preferred_element_type=F32)
    high = total.astype(BF16).astype(F32)
    low = total - high
    top = jnp.broadcast_to(top, context.shape)
    high = jnp.broadcast_to(high, context.shape)
    low = jnp.broadcast_to(low, context.shape)
    lat_t = lat.T
    rot_t = rot.astype(F32).T
    for t in range(out_ref.shape[0]):
        slot = out_ref.shape[0] - 1 - t
        out_ref[slot, 0:64, :] = lat_t[64 * t : 64 * (t + 1)]
        mine = slice(2 * t, 2 * t + 2)
        block = jnp.concatenate(
            [rot_t[8 * t : 8 * t + 8], context[mine], top[mine], high[mine], low[mine]], axis=0
        )
        out_ref[slot, 64:80, :] = block.astype(BF16)


def finish_kernel(y_ref, w_ref, st_ref, rt_ref, fr_ref):
    count = y_ref.shape[0]
    for q in range(4):
        for o in range(4):
            for j in range(2):
                lanes = slice((4 * q + o) * 32, (4 * q + o) * 32 + 32)
                tile = jnp.concatenate(
                    [y_ref[count - 1 - (4 * j + k), 0:80, lanes] for k in range(4)], axis=1
                )
                at = (4 * q + o) * 256 + j * 128
                st_ref[:, at : at + 128] = tile[0:64]
                rt_ref[:, at : at + 128] = tile[64:72]
    tails = [y_ref[t, 64:80, :].astype(F32)[8:16] for t in range(count)]
    tops = [v[2:4] for v in tails]
    peak = tops[0]
    for v in tops[1:]:
        peak = jnp.maximum(peak, v)
    number = jnp.zeros_like(peak)
    denominator = jnp.zeros_like(peak)
    for v, top in zip(tails, tops):
        scale = jnp.exp(top - peak)
        number = number + scale * v[0:2]
        denominator = denominator + scale * (v[4:6] + v[6:8])
    context = (number / denominator).astype(BF16)
    weight = jnp.concatenate([w_ref[count - 1 - t, 0:64, :] for t in range(count)], axis=0)
    values = jnp.dot(context, weight, preferred_element_type=F32)
    values = jnp.concatenate([values[0:1, 0:128], values[1:2, 128:256]], axis=0)
    mean = jnp.mean(values * values, axis=-1, keepdims=True)
    fr_ref[...] = (values * lax.rsqrt(mean + norm_eps)).astype(BF16)


def groups_of(sp, tp, over_sp):
    if over_sp:
        return [[s * tp + t for s in reversed(range(sp))] for t in range(tp)]
    return [[s * tp + t for t in reversed(range(tp))] for s in range(sp)]


def exchange(array, sp, tp, over_sp):
    groups = groups_of(sp, tp, over_sp)
    return lax.all_to_all(array, SP_TP, 0, 0, tiled=True, axis_index_groups=groups)


def in_hbm(array):
    return pltpu.with_memory_space_constraint(array, pltpu.HBM)


def call(kernel, out_shape, flops, moved, **kwargs):
    return pl.pallas_call(
        kernel,
        out_shape=out_shape,
        **kwargs,
        cost_estimate=pl.CostEstimate(flops=flops, bytes_accessed=moved, transcendentals=0),
        compiler_params=pltpu.CompilerParams(vmem_limit_bytes=32 * 1024 * 1024),
    )


def shards(
    layer_input,
    input_gain,
    narrowing_matrix,
    rotary_down,
    summary_scaling,
    lookup_widening,
    payload_widening,
    query_nope,
    query_rotary,
):
    seqs, pos_local, width = layer_input.shape
    tp = lax.axis_size(TP)
    sp = lax.axis_size("sp")
    me = lax.axis_index(TP)
    block = lax.axis_index(SP_TP)
    shape = jax.ShapeDtypeStruct

    lookup_other = lax.ppermute(lookup_widening, "c", [(0, 1), (1, 0)])
    flat = in_hbm(layer_input.reshape(seqs * pos_local, width))
    packed, first_rows = call(
        pack_weights_kernel,
        (shape((tp, 80, 256), BF16), shape((FIRST_ROWS, width), BF16)),
        30_000_000_000,
        60_000_000,
        in_specs=[pl.BlockSpec(memory_space=pltpu.HBM)] * 4,
        scratch_shapes=[
            pltpu.VMEM(payload_widening.shape, BF16),
            pltpu.VMEM(query_nope.shape[1:], BF16),
            pltpu.VMEM(query_rotary.shape[1:], BF16),
            pltpu.SemaphoreType.DMA((4,)),
        ],
    )(
        in_hbm(payload_widening),
        in_hbm(query_nope[0]),
        in_hbm(query_rotary[0]),
        flat,
    )
    spread = exchange(packed, sp, tp, False)

    positions = (block * pos_local + jnp.arange(pos_local, dtype=jnp.int32)).astype(F32)
    angles = positions[:, None] * frequencies()[None, :]
    cos, sin = jnp.cos(angles), jnp.sin(angles)
    table = jnp.stack(
        [jnp.concatenate([cos, cos], axis=1), jnp.concatenate([-sin, sin], axis=1)]
    )
    whole = pl.BlockSpec(memory_space=pltpu.VMEM)
    sent = call(
        project_kernel,
        shape((seqs, pos_local, 640), BF16),
        1_300_000_000,
        5_000_000,
        in_specs=[whole, pl.BlockSpec(memory_space=pltpu.HBM)] + [whole] * 5,
        scratch_shapes=[
            pltpu.VMEM((seqs * pos_local - FIRST_ROWS, width), BF16),
            pltpu.SemaphoreType.DMA(()),
        ],
    )(first_rows, flat, input_gain[None], narrowing_matrix, rotary_down.T, summary_scaling[None], table)
    held = exchange(sent, sp, tp, True)

    query = spread[::-1, 64, :].reshape(2 * tp, 128)
    turn = spread[::-1, 65, 0:128].reshape(2 * tp, QK_ROPE)
    lane = lax.broadcasted_iota(jnp.int32, (2 * tp, 512), 1) // 64
    placed = jnp.zeros((), BF16)
    for owner, weight in ((me, lookup_widening), (me ^ 1, lookup_other)):
        share = jnp.einsum("hd,chd->hc", query, weight, preferred_element_type=F32)
        share = jnp.concatenate([share.astype(BF16)] * tp, axis=1)
        placed = placed + jnp.where(lane == owner, share, jnp.zeros((), BF16))
    moved = lax.ppermute(placed, "x", [(0, 1), (1, 0), (2, 3), (3, 2)])
    placed = placed + moved
    other = lax.ppermute(placed, "x", [(0, 3), (3, 0), (1, 2), (2, 1)])
    turned = rotate(turn.astype(F32), F32(seqs * 0 + sp * tp * pos_local)).astype(BF16)
    turned = jnp.concatenate([turned, jnp.zeros_like(turned)], axis=1)

    piece = call(attend_kernel, shape((tp, 80, 512), BF16), 600_000_000, 1_300_000)(
        held, placed, other, turned
    )
    arrived = exchange(piece, sp, tp, False)

    total = sp * tp * pos_local
    stored, rotary, first = call(
        finish_kernel,
        (shape((64, total), BF16), shape((8, total), BF16), shape((2, 128), BF16)),
        10_000_000,
        1_800_000,
    )(arrived, spread)
    return stored.T[None], rotary.T[None], first[None]


def solution(mesh):
    torus = Mesh(mesh.devices.reshape(mesh.shape["sp"], 4, 2), SP_TP)
    in_specs = (
        P(None, SP_TP, None),
        P(),
        P(),
        P(),
        P(),
        P(TP, None, None),
        P(TP, None, None),
        P("sp", TP, None),
        P("sp", TP, None),
    )
    out_specs = (P("sp", None, TP), P("sp", None, TP), P("sp", TP, None))

    return jax.shard_map(
        shards, mesh=torus, in_specs=in_specs, out_specs=out_specs, check_vma=False
    )
```

```python
import jax
import jax.numpy as jnp
from jax import lax
from jax.experimental import pallas as pl
from jax.experimental.pallas import tpu as pltpu
from jax.sharding import Mesh
from jax.sharding import PartitionSpec as P

QK_ROPE = 64
PLAIN_MATCH_SPAN = 128
TP = ("x", "c")
SP_TP = ("sp", "x", "c")

norm_eps = 1e-06
rotary_base = 10000.0
F32 = jnp.float32
BF16 = jnp.bfloat16
LAST = (((1,), (1,)), ((), ()))


def frequencies():
    half = QK_ROPE // 2
    return 1.0 / rotary_base ** (jnp.arange(half, dtype=F32) * 2.0 / QK_ROPE)


def rotate(vector, position):
    half_width = vector.shape[-1] // 2
    angles = position * frequencies()
    first_half = vector[..., :half_width]
    second_half = vector[..., half_width:]
    return jnp.concatenate(
        [
            first_half * jnp.cos(angles) - second_half * jnp.sin(angles),
            second_half * jnp.cos(angles) + first_half * jnp.sin(angles),
        ],
        axis=-1,
    )


def place_queries_kernel(at_ref, mine_ref, partner_ref, out_ref):
    mine = mine_ref[...].astype(F32)
    partner = partner_ref[...].astype(F32)
    first = jnp.where(at_ref[1] == 0, mine, partner)
    second = jnp.where(at_ref[1] == 0, partner, mine)
    rows = jnp.concatenate([first, second] * 4, axis=0)
    row = lax.broadcasted_iota(jnp.int32, rows.shape, 0) // 4
    out_ref[...] = jnp.where(row == at_ref[0], rows, 0.0).astype(BF16)


def pack_payload_kernel(at_ref, own_ref, other_ref, *refs):
    outs, (own_f32, other_f32) = refs[:4], refs[4:]
    heads = own_ref.shape[1]
    own_f32[...] = own_ref[...].astype(F32).reshape(own_f32.shape)
    other_f32[...] = other_ref[...].astype(F32).reshape(other_f32.shape)
    for d, out_ref in enumerate(outs):
        first = 2 * (2 * ((at_ref[0] + d) % 4) + at_ref[1])
        for r, source in enumerate((own_f32, other_f32)):
            for h in range(2):
                rows = source[pl.ds(first + h, out_ref.shape[1], stride=heads), :]
                out_ref[r, :, h * 128 : (h + 1) * 128] = rows.astype(BF16)


def project_kernel(x_ref, gain_ref, w_ref, r_ref, scal_ref, cs_ref, out_ref):
    rows = x_ref.shape[0]
    step = 128
    gain = gain_ref[...]
    scal = scal_ref[...]
    seqs = step // 32
    cos = jnp.concatenate([cs_ref[0]] * seqs, axis=0)
    sin = jnp.concatenate([cs_ref[1]] * seqs, axis=0)
    for i in range(rows // step):
        x = x_ref[i * step : (i + 1) * step, :].astype(F32)
        mean = jnp.mean(x * x, axis=-1, keepdims=True)
        normed = (x * lax.rsqrt(mean + norm_eps) * gain).astype(BF16)
        lat = jnp.dot(normed, w_ref[...], preferred_element_type=F32).astype(BF16).astype(F32)
        rot = lax.dot_general(normed, r_ref[...], LAST, preferred_element_type=F32)
        rot = rot.astype(BF16).astype(F32)
        mean = jnp.mean(lat * lat, axis=-1, keepdims=True)
        lat = (lat * lax.rsqrt(mean + norm_eps) * scal).astype(BF16)
        swapped = jnp.concatenate([rot[:, 32:], rot[:, :32]], axis=1)
        rot = rot * cos + swapped * sin
        rot = jnp.concatenate([rot, jnp.zeros_like(rot)], axis=1).astype(BF16)
        for s in range(seqs):
            slot = out_ref.shape[0] - 1 - (i * seqs + s)
            out_ref[slot, :, 0:512] = lat[s * 32 : (s + 1) * 32]
            out_ref[slot, :, 512:640] = rot[s * 32 : (s + 1) * 32]


def attend_kernel(z_ref, a0_ref, a1_ref, t_ref, out_ref):
    order = range(z_ref.shape[0] - 1, -1, -1)
    lat = jnp.concatenate([z_ref[i, :, 0:512] for i in order], axis=0)
    rot = jnp.concatenate([z_ref[i, :, 512:640] for i in order], axis=0)
    absorbed = a0_ref[...] + a1_ref[...]
    scores = lax.dot_general(absorbed, lat, LAST, preferred_element_type=F32)
    scores = scores + lax.dot_general(t_ref[...], rot, LAST, preferred_element_type=F32)
    scores = scores * ((PLAIN_MATCH_SPAN + QK_ROPE) ** (-0.5))
    top = jnp.max(scores, axis=-1, keepdims=True).astype(BF16).astype(F32)
    weight = jnp.exp(scores - top)
    total = jnp.sum(weight, axis=-1, keepdims=True)
    context = jnp.dot(weight.astype(BF16), lat, preferred_element_type=F32)
    high = total.astype(BF16).astype(F32)
    low = total - high
    top = jnp.broadcast_to(top, context.shape)
    high = jnp.broadcast_to(high, context.shape)
    low = jnp.broadcast_to(low, context.shape)
    lat_t = lat.T
    rot_t = rot.astype(F32).T
    for t in range(out_ref.shape[0]):
        slot = out_ref.shape[0] - 1 - t
        out_ref[slot, 0:64, :] = lat_t[64 * t : 64 * (t + 1)]
        mine = slice(2 * t, 2 * t + 2)
        block = jnp.concatenate(
            [rot_t[8 * t : 8 * t + 8], context[mine], top[mine], high[mine], low[mine]], axis=0
        )
        out_ref[slot, 64:80, :] = block.astype(BF16)


def order_payload_kernel(at_ref, p0_ref, p1_ref, p2_ref, p3_ref, out_ref):
    for d, piece in enumerate((p0_ref, p1_ref, p2_ref, p3_ref)):
        chip = (at_ref[0] + 4 - d) % 4
        out_ref[2 * chip + at_ref[1]] = piece[0]
        out_ref[2 * chip + 1 - at_ref[1]] = piece[1]


def finish_kernel(y_ref, w_ref, st_ref, rt_ref, fr_ref):
    count = y_ref.shape[0]
    for q in range(4):
        for o in range(4):
            for j in range(2):
                lanes = slice((4 * q + o) * 32, (4 * q + o) * 32 + 32)
                tile = jnp.concatenate(
                    [y_ref[count - 1 - (4 * j + k), 0:80, lanes] for k in range(4)], axis=1
                )
                at = (4 * q + o) * 256 + j * 128
                st_ref[:, at : at + 128] = tile[0:64]
                rt_ref[:, at : at + 128] = tile[64:72]
    tails = [y_ref[t, 64:80, :].astype(F32)[8:16] for t in range(count)]
    tops = [v[2:4] for v in tails]
    peak = tops[0]
    for v in tops[1:]:
        peak = jnp.maximum(peak, v)
    number = jnp.zeros_like(peak)
    denominator = jnp.zeros_like(peak)
    for v, top in zip(tails, tops):
        scale = jnp.exp(top - peak)
        number = number + scale * v[0:2]
        denominator = denominator + scale * (v[4:6] + v[6:8])
    context = (number / denominator).astype(BF16)
    weight = w_ref[...].reshape(count * 64, 256)
    values = jnp.dot(context, weight, preferred_element_type=F32)
    values = jnp.concatenate([values[0:1, 0:128], values[1:2, 128:256]], axis=0)
    mean = jnp.mean(values * values, axis=-1, keepdims=True)
    fr_ref[...] = (values * lax.rsqrt(mean + norm_eps)).astype(BF16)


def exchange(array, sp, tp, over_sp):
    if over_sp:
        groups = [[s * tp + t for s in reversed(range(sp))] for t in range(tp)]
    else:
        groups = [[s * tp + t for t in reversed(range(tp))] for s in range(sp)]
    return lax.all_to_all(array, SP_TP, 0, 0, tiled=True, axis_index_groups=groups)


def call(kernel, out_shape, flops, moved, **kwargs):
    return pl.pallas_call(
        kernel,
        out_shape=out_shape,
        **kwargs,
        cost_estimate=pl.CostEstimate(flops=flops, bytes_accessed=moved, transcendentals=0),
        compiler_params=pltpu.CompilerParams(vmem_limit_bytes=32 * 1024 * 1024),
    )


def shards(
    layer_input,
    input_gain,
    narrowing_matrix,
    rotary_down,
    summary_scaling,
    lookup_widening,
    payload_widening,
    query_nope,
    query_rotary,
):
    seqs, pos_local, width = layer_input.shape
    tp = lax.axis_size(TP)
    sp = lax.axis_size("sp")
    block = lax.axis_index(SP_TP)
    shape = jax.ShapeDtypeStruct

    at = jnp.stack([lax.axis_index("x"), lax.axis_index("c")]).astype(jnp.int32)
    small = pl.BlockSpec(memory_space=pltpu.SMEM)
    whole = pl.BlockSpec(memory_space=pltpu.VMEM)
    outside = pl.BlockSpec(memory_space=pltpu.HBM)
    swap = [(0, 1), (1, 0)]
    lookup_other = lax.ppermute(lookup_widening, "c", swap)
    payload_other = lax.ppermute(payload_widening, "c", swap)
    mine = jnp.concatenate(
        [query_nope[0], query_rotary[0], jnp.zeros_like(query_rotary[0])], axis=1
    )
    partner = lax.ppermute(mine, "c", swap)
    query = call(
        place_queries_kernel,
        shape((2 * tp, 256), BF16),
        30_000_000_000,
        60_000_000,
        in_specs=[small, whole, whole],
    )(at, mine, partner)
    near, far = [(0, 1), (1, 0), (2, 3), (3, 2)], [(0, 3), (3, 0), (1, 2), (2, 1)]
    moved = lax.ppermute(query, "x", near)
    query = query + moved
    moved = lax.ppermute(query, "x", far)

    positions = (block * pos_local + jnp.arange(pos_local, dtype=jnp.int32)).astype(F32)
    angles = positions[:, None] * frequencies()[None, :]
    cos, sin = jnp.cos(angles), jnp.sin(angles)
    table = jnp.stack(
        [jnp.concatenate([cos, cos], axis=1), jnp.concatenate([-sin, sin], axis=1)]
    )
    sent = call(
        project_kernel,
        shape((seqs, pos_local, 640), BF16),
        1_300_000_000,
        5_000_000,
    )(
        layer_input.reshape(seqs * pos_local, width),
        input_gain[None],
        narrowing_matrix,
        rotary_down.T,
        summary_scaling[None],
        table,
    )
    held = exchange(sent, sp, tp, True)

    query = query + moved
    turn = query[:, 128 : 128 + QK_ROPE]
    query = query[:, :128]
    own, partner = (
        jnp.einsum("hd,chd->hc", query, weight, preferred_element_type=F32).astype(BF16)
        for weight in (lookup_widening, lookup_other)
    )
    first, second = jnp.where(at[1] == 0, own, partner), jnp.where(at[1] == 0, partner, own)
    share = jnp.concatenate([first, second] * 4, axis=1)
    lane = lax.broadcasted_iota(jnp.int32, (2 * tp, 512), 1) // 128
    placed = jnp.where(lane == at[0], share, jnp.zeros((), BF16))
    moved = lax.ppermute(placed, "x", near)
    placed = placed + moved
    other = lax.ppermute(placed, "x", far)
    each = payload_widening.shape[0]
    parts = call(
        pack_payload_kernel,
        [shape((2, each, 256), BF16)] * 4,
        1_000_000,
        1_000_000,
        in_specs=[small, whole, whole],
        scratch_shapes=[pltpu.VMEM((each * 2 * tp, 128), F32)] * 2,
    )(at, payload_widening, payload_other)
    pieces = [parts[0]]
    for d in (1, 2, 3):
        pieces.append(lax.ppermute(parts[d], "x", [(i, (i + d) % 4) for i in range(4)]))
    turned = rotate(turn.astype(F32), F32(seqs * 0 + sp * tp * pos_local)).astype(BF16)
    turned = jnp.concatenate([turned, jnp.zeros_like(turned)], axis=1)

    piece = call(attend_kernel, shape((tp, 80, 512), BF16), 600_000_000, 1_300_000)(
        held, placed, other, turned
    )
    arrived = exchange(piece, sp, tp, False)
    weight = call(
        order_payload_kernel,
        shape((tp, each, 256), BF16),
        1_000_000,
        500_000,
        in_specs=[small] + [whole] * 4,
    )(at, *pieces)

    total = sp * tp * pos_local
    stored, rotary, first = call(
        finish_kernel,
        (shape((64, total), BF16), shape((8, total), BF16), shape((2, 128), BF16)),
        10_000_000,
        1_800_000,
    )(arrived, weight)
    return stored.T[None], rotary.T[None], first[None]


def solution(mesh):
    torus = Mesh(mesh.devices.reshape(mesh.shape["sp"], 4, 2), SP_TP)
    in_specs = (
        P(None, SP_TP, None),
        P(),
        P(),
        P(),
        P(),
        P(TP, None, None),
        P(TP, None, None),
        P("sp", TP, None),
        P("sp", TP, None),
    )
    out_specs = (P("sp", None, TP), P("sp", None, TP), P("sp", TP, None))

    return jax.shard_map(
        shards, mesh=torus, in_specs=in_specs, out_specs=out_specs, check_vma=False
    )
```

```python
import jax
import jax.numpy as jnp
from jax import lax
from jax.experimental import pallas as pl
from jax.experimental.pallas import tpu as pltpu
from jax.sharding import Mesh
from jax.sharding import PartitionSpec as P

QK_ROPE = 64
PLAIN_MATCH_SPAN = 128
TP = ("x", "c")
SP_TP = ("sp", "x", "c")

norm_eps = 1e-06
rotary_base = 10000.0
F32 = jnp.float32
BF16 = jnp.bfloat16
LAST = (((1,), (1,)), ((), ()))


def frequencies():
    half = QK_ROPE // 2
    return 1.0 / rotary_base ** (jnp.arange(half, dtype=F32) * 2.0 / QK_ROPE)


def rotate(vector, position):
    half_width = vector.shape[-1] // 2
    angles = position * frequencies()
    first_half = vector[..., :half_width]
    second_half = vector[..., half_width:]
    return jnp.concatenate(
        [
            first_half * jnp.cos(angles) - second_half * jnp.sin(angles),
            second_half * jnp.cos(angles) + first_half * jnp.sin(angles),
        ],
        axis=-1,
    )


def place_queries_kernel(at_ref, mine_ref, partner_ref, out_ref):
    mine = mine_ref[...].astype(F32)
    partner = partner_ref[...].astype(F32)
    first = jnp.where(at_ref[1] == 0, mine, partner)
    second = jnp.where(at_ref[1] == 0, partner, mine)
    rows = jnp.concatenate([first, second] * 4, axis=0)
    row = lax.broadcasted_iota(jnp.int32, rows.shape, 0) // 4
    out_ref[...] = jnp.where(row == at_ref[0], rows, 0.0).astype(BF16)


def pack_payload_kernel(at_ref, own_ref, other_ref, *refs):
    outs, (own_f32, other_f32) = refs[:4], refs[4:]
    heads = own_ref.shape[1]
    own_f32[...] = own_ref[...].astype(F32).reshape(own_f32.shape)
    other_f32[...] = other_ref[...].astype(F32).reshape(other_f32.shape)
    for d, out_ref in enumerate(outs):
        first = 2 * (2 * ((at_ref[0] + d) % 4) + at_ref[1])
        for r, source in enumerate((own_f32, other_f32)):
            for h in range(2):
                rows = source[pl.ds(first + h, out_ref.shape[1], stride=heads), :]
                out_ref[r, :, h * 128 : (h + 1) * 128] = rows.astype(BF16)


def project_kernel(x_ref, gain_ref, w_ref, r_ref, scal_ref, cs_ref, out_ref):
    count = out_ref.shape[0]
    x = x_ref[...].astype(F32)
    scale = lax.rsqrt(jnp.mean(x * x, axis=-1, keepdims=True) + norm_eps)
    gained = (x * gain_ref[...]).astype(BF16)
    lat = jnp.dot(gained, w_ref[...], preferred_element_type=F32)
    rot = lax.dot_general(gained, r_ref[...], LAST, preferred_element_type=F32)
    lat = (lat * scale).astype(BF16).astype(F32)
    rot = (rot * scale).astype(BF16).astype(F32)
    mean = jnp.mean(lat * lat, axis=-1, keepdims=True)
    lat = (lat * lax.rsqrt(mean + norm_eps) * scal_ref[...]).astype(BF16)
    cos = jnp.concatenate([cs_ref[0]] * count, axis=0)
    sin = jnp.concatenate([cs_ref[1]] * count, axis=0)
    swapped = jnp.concatenate([rot[:, 32:], rot[:, :32]], axis=1)
    rot = rot * cos + swapped * sin
    for s in range(count):
        slot = count - 1 - s
        at = s * 32
        pair = jnp.concatenate([rot[at : at + 16], rot[at + 16 : at + 32]], axis=1)
        out_ref[slot, :, 0:512] = lat[at : at + 16]
        out_ref[slot, :, 512:1024] = lat[at + 16 : at + 32]
        out_ref[slot, :, 1024:1152] = pair.astype(BF16)


def attend_kernel(z_ref, a0_ref, a1_ref, t_ref, out_ref):
    lats, rots = [], []
    for i in range(z_ref.shape[0] - 1, -1, -1):
        lats += [z_ref[i, :, 0:512], z_ref[i, :, 512:1024]]
        pair = z_ref[i, :, 1024:1152]
        rots += [pair, jnp.concatenate([pair[:, 64:], pair[:, :64]], axis=1)]
    lat = jnp.concatenate(lats, axis=0)
    rot = jnp.concatenate(rots, axis=0)
    absorbed = a0_ref[...] + a1_ref[...]
    scores = lax.dot_general(absorbed, lat, LAST, preferred_element_type=F32)
    scores = scores + lax.dot_general(t_ref[...], rot, LAST, preferred_element_type=F32)
    scores = scores * ((PLAIN_MATCH_SPAN + QK_ROPE) ** (-0.5))
    top = jnp.max(scores, axis=-1, keepdims=True).astype(BF16).astype(F32)
    weight = jnp.exp(scores - top)
    total = jnp.sum(weight, axis=-1, keepdims=True)
    context = jnp.dot(weight.astype(BF16), lat, preferred_element_type=F32)
    high = total.astype(BF16).astype(F32)
    low = total - high
    top = jnp.broadcast_to(top, context.shape)
    high = jnp.broadcast_to(high, context.shape)
    low = jnp.broadcast_to(low, context.shape)
    lat_t = lat.T
    rot_t = rot.astype(F32).T
    for t in range(out_ref.shape[0]):
        slot = out_ref.shape[0] - 1 - t
        out_ref[slot, 0:64, :] = lat_t[64 * t : 64 * (t + 1)]
        mine = slice(2 * t, 2 * t + 2)
        block = jnp.concatenate(
            [rot_t[8 * t : 8 * t + 8], context[mine], top[mine], high[mine], low[mine]], axis=0
        )
        out_ref[slot, 64:80, :] = block.astype(BF16)


def order_payload_kernel(at_ref, p0_ref, p1_ref, p2_ref, p3_ref, out_ref):
    for d, piece in enumerate((p0_ref, p1_ref, p2_ref, p3_ref)):
        chip = (at_ref[0] + 4 - d) % 4
        out_ref[2 * chip + at_ref[1]] = piece[0]
        out_ref[2 * chip + 1 - at_ref[1]] = piece[1]


def finish_kernel(y_ref, w_ref, st_ref, rt_ref, fr_ref):
    count = y_ref.shape[0]
    for q in range(4):
        for o in range(4):
            for j in range(2):
                lanes = slice((4 * q + o) * 32, (4 * q + o) * 32 + 32)
                tile = jnp.concatenate(
                    [y_ref[count - 1 - (4 * j + k), 0:80, lanes] for k in range(4)], axis=1
                )
                at = (4 * q + o) * 256 + j * 128
                st_ref[:, at : at + 128] = tile[0:64]
                rt_ref[:, at : at + 128] = tile[64:72]
    tails = [y_ref[t, 64:80, :].astype(F32)[8:16] for t in range(count)]
    tops = [v[2:4] for v in tails]
    peak = tops[0]
    for v in tops[1:]:
        peak = jnp.maximum(peak, v)
    number = jnp.zeros_like(peak)
    denominator = jnp.zeros_like(peak)
    for v, top in zip(tails, tops):
        scale = jnp.exp(top - peak)
        number = number + scale * v[0:2]
        denominator = denominator + scale * (v[4:6] + v[6:8])
    context = (number / denominator).astype(BF16)
    weight = w_ref[...].reshape(count * 64, 256)
    values = jnp.dot(context, weight, preferred_element_type=F32)
    values = jnp.concatenate([values[0:1, 0:128], values[1:2, 128:256]], axis=0)
    mean = jnp.mean(values * values, axis=-1, keepdims=True)
    fr_ref[...] = (values * lax.rsqrt(mean + norm_eps)).astype(BF16)


def exchange(array, sp, tp, over_sp):
    if over_sp:
        groups = [[s * tp + t for s in reversed(range(sp))] for t in range(tp)]
    else:
        groups = [[s * tp + t for t in reversed(range(tp))] for s in range(sp)]
    return lax.all_to_all(array, SP_TP, 0, 0, tiled=True, axis_index_groups=groups)


def call(kernel, out_shape, flops, moved, **kwargs):
    return pl.pallas_call(
        kernel,
        out_shape=out_shape,
        **kwargs,
        cost_estimate=pl.CostEstimate(flops=flops, bytes_accessed=moved, transcendentals=0),
        compiler_params=pltpu.CompilerParams(vmem_limit_bytes=32 * 1024 * 1024),
    )


def shards(
    layer_input,
    input_gain,
    narrowing_matrix,
    rotary_down,
    summary_scaling,
    lookup_widening,
    payload_widening,
    query_nope,
    query_rotary,
):
    seqs, pos_local, width = layer_input.shape
    tp = lax.axis_size(TP)
    sp = lax.axis_size("sp")
    block = lax.axis_index(SP_TP)
    shape = jax.ShapeDtypeStruct

    at = jnp.stack([lax.axis_index("x"), lax.axis_index("c")]).astype(jnp.int32)
    small = pl.BlockSpec(memory_space=pltpu.SMEM)
    whole = pl.BlockSpec(memory_space=pltpu.VMEM)
    outside = pl.BlockSpec(memory_space=pltpu.HBM)
    swap = [(0, 1), (1, 0)]
    lookup_other = lax.ppermute(lookup_widening, "c", swap)
    payload_other = lax.ppermute(payload_widening, "c", swap)
    mine = jnp.concatenate(
        [query_nope[0], query_rotary[0], jnp.zeros_like(query_rotary[0])], axis=1
    )
    partner = lax.ppermute(mine, "c", swap)
    query = call(
        place_queries_kernel,
        shape((2 * tp, 256), BF16),
        30_000_000_000,
        60_000_000,
        in_specs=[small, whole, whole],
    )(at, mine, partner)
    near, far = [(0, 1), (1, 0), (2, 3), (3, 2)], [(0, 3), (3, 0), (1, 2), (2, 1)]
    moved = lax.ppermute(query, "x", far)
    query = query + moved
    moved = lax.ppermute(query, "x", near)

    positions = (block * pos_local + jnp.arange(pos_local, dtype=jnp.int32)).astype(F32)
    angles = positions[:, None] * frequencies()[None, :]
    cos, sin = jnp.cos(angles), jnp.sin(angles)
    table = jnp.stack(
        [jnp.concatenate([cos, cos], axis=1), jnp.concatenate([-sin, sin], axis=1)]
    )
    sent = call(
        project_kernel,
        shape((seqs, pos_local // 2, 1152), BF16),
        1_300_000_000,
        5_000_000,
    )(
        layer_input.reshape(seqs * pos_local, width),
        input_gain[None],
        narrowing_matrix,
        rotary_down.T,
        summary_scaling[None],
        table,
    )
    held = exchange(sent, sp, tp, True)

    query = query + moved
    turn = query[:, 128 : 128 + QK_ROPE]
    query = query[:, :128]
    own, partner = (
        jnp.einsum("hd,chd->hc", query, weight, preferred_element_type=F32).astype(BF16)
        for weight in (lookup_widening, lookup_other)
    )
    first, second = jnp.where(at[1] == 0, own, partner), jnp.where(at[1] == 0, partner, own)
    share = jnp.concatenate([first, second] * 4, axis=1)
    lane = lax.broadcasted_iota(jnp.int32, (2 * tp, 512), 1) // 128
    placed = jnp.where(lane == at[0], share, jnp.zeros((), BF16))
    moved = lax.ppermute(placed, "x", near)
    placed = placed + moved
    other = lax.ppermute(placed, "x", far)
    each = payload_widening.shape[0]
    parts = call(
        pack_payload_kernel,
        [shape((2, each, 256), BF16)] * 4,
        1_000_000,
        1_000_000,
        in_specs=[small, whole, whole],
        scratch_shapes=[pltpu.VMEM((each * 2 * tp, 128), F32)] * 2,
    )(at, payload_widening, payload_other)
    pieces = [parts[0]]
    for d in (1, 2, 3):
        pieces.append(lax.ppermute(parts[d], "x", [(i, (i + d) % 4) for i in range(4)]))
    turned = rotate(turn.astype(F32), F32(seqs * 0 + sp * tp * pos_local)).astype(BF16)
    turned = jnp.concatenate([turned, jnp.zeros_like(turned)], axis=1)

    piece = call(attend_kernel, shape((tp, 80, 512), BF16), 600_000_000, 1_300_000)(
        held, placed, other, turned
    )
    arrived = exchange(piece, sp, tp, False)
    weight = call(
        order_payload_kernel,
        shape((tp, each, 256), BF16),
        1_000_000,
        500_000,
        in_specs=[small] + [whole] * 4,
    )(at, *pieces)

    total = sp * tp * pos_local
    stored, rotary, first = call(
        finish_kernel,
        (shape((64, total), BF16), shape((8, total), BF16), shape((2, 128), BF16)),
        10_000_000,
        1_800_000,
    )(arrived, weight)
    return stored.T[None], rotary.T[None], first[None]


def solution(mesh):
    torus = Mesh(mesh.devices.reshape(mesh.shape["sp"], 4, 2), SP_TP)
    in_specs = (
        P(None, SP_TP, None),
        P(),
        P(),
        P(),
        P(),
        P(TP, None, None),
        P(TP, None, None),
        P("sp", TP, None),
        P("sp", TP, None),
    )
    out_specs = (P("sp", None, TP), P("sp", None, TP), P("sp", TP, None))

    return jax.shard_map(
        shards, mesh=torus, in_specs=in_specs, out_specs=out_specs, check_vma=False
    )
```

```python
import jax
import jax.numpy as jnp
from jax import lax
from jax.experimental import pallas as pl
from jax.experimental.pallas import tpu as pltpu
from jax.sharding import Mesh
from jax.sharding import PartitionSpec as P

QK_ROPE = 64
PLAIN_MATCH_SPAN = 128
TP = ("x", "c")
SP_TP = ("sp", "x", "c")

norm_eps = 1e-06
rotary_base = 10000.0
F32 = jnp.float32
BF16 = jnp.bfloat16
LAST = (((1,), (1,)), ((), ()))


def frequencies():
    half = QK_ROPE // 2
    return 1.0 / rotary_base ** (jnp.arange(half, dtype=F32) * 2.0 / QK_ROPE)


def rotate(vector, position):
    half_width = vector.shape[-1] // 2
    angles = position * frequencies()
    first_half = vector[..., :half_width]
    second_half = vector[..., half_width:]
    return jnp.concatenate(
        [
            first_half * jnp.cos(angles) - second_half * jnp.sin(angles),
            second_half * jnp.cos(angles) + first_half * jnp.sin(angles),
        ],
        axis=-1,
    )


def table_kernel(freq_ref, out_ref):
    rows, lanes = out_ref.shape[1:]
    first = lax.axis_index(SP_TP) * rows
    position = first + lax.broadcasted_iota(jnp.int32, (rows, lanes), 0)
    angles = position.astype(F32) * freq_ref[...]
    lane = lax.broadcasted_iota(jnp.int32, (rows, lanes), 1)
    sin = jnp.sin(angles)
    out_ref[0] = jnp.cos(angles)
    out_ref[1] = jnp.where(lane < lanes // 2, -sin, sin)


def place_queries_kernel(qn_ref, qr_ref, qn_other_ref, qr_other_ref, out_ref):
    blank = jnp.zeros(qr_ref.shape, F32)
    mine = jnp.concatenate([qn_ref[...].astype(F32), qr_ref[...].astype(F32), blank], axis=1)
    partner = jnp.concatenate(
        [qn_other_ref[...].astype(F32), qr_other_ref[...].astype(F32), blank], axis=1
    )
    core = lax.axis_index("c")
    first = jnp.where(core == 0, mine, partner)
    second = jnp.where(core == 0, partner, mine)
    rows = jnp.concatenate([first, second] * 4, axis=0)
    row = lax.broadcasted_iota(jnp.int32, rows.shape, 0) // 4
    out_ref[...] = jnp.where(row == lax.axis_index("x"), rows, 0.0).astype(BF16)


def pack_payload_kernel(own_ref, other_ref, *refs):
    x, core = lax.axis_index("x"), lax.axis_index("c")
    outs, (own_f32, other_f32) = refs[:4], refs[4:]
    heads = own_ref.shape[1]
    own_f32[...] = own_ref[...].astype(F32).reshape(own_f32.shape)
    other_f32[...] = other_ref[...].astype(F32).reshape(other_f32.shape)
    for d, out_ref in enumerate(outs):
        first = 2 * (2 * ((x + d) % 4) + core)
        for r, source in enumerate((own_f32, other_f32)):
            for h in range(2):
                rows = source[pl.ds(first + h, out_ref.shape[1], stride=heads), :]
                out_ref[r, :, h * 128 : (h + 1) * 128] = rows.astype(BF16)


def project_kernel(x_ref, gain_ref, w_ref, r_ref, scal_ref, cs_ref, out_ref):
    count = out_ref.shape[0]
    x = x_ref[...].astype(F32)
    scale = lax.rsqrt(jnp.mean(x * x, axis=-1, keepdims=True) + norm_eps)
    gained = (x * gain_ref[...]).astype(BF16)
    lat = jnp.dot(gained, w_ref[...], preferred_element_type=F32)
    rot = lax.dot_general(gained, r_ref[...], LAST, preferred_element_type=F32)
    lat = (lat * scale).astype(BF16).astype(F32)
    rot = (rot * scale).astype(BF16).astype(F32)
    mean = jnp.mean(lat * lat, axis=-1, keepdims=True)
    lat = (lat * lax.rsqrt(mean + norm_eps) * scal_ref[...]).astype(BF16)
    cos = jnp.concatenate([cs_ref[0]] * count, axis=0)
    sin = jnp.concatenate([cs_ref[1]] * count, axis=0)
    swapped = jnp.concatenate([rot[:, 32:], rot[:, :32]], axis=1)
    rot = rot * cos + swapped * sin
    for s in range(count):
        slot = count - 1 - s
        at = s * 32
        pair = jnp.concatenate([rot[at : at + 16], rot[at + 16 : at + 32]], axis=1)
        out_ref[slot, :, 0:512] = lat[at : at + 16]
        out_ref[slot, :, 512:1024] = lat[at + 16 : at + 32]
        out_ref[slot, :, 1024:1152] = pair.astype(BF16)


def attend_kernel(z_ref, a0_ref, a1_ref, t_ref, out_ref):
    lats, rots = [], []
    for i in range(z_ref.shape[0] - 1, -1, -1):
        lats += [z_ref[i, :, 0:512], z_ref[i, :, 512:1024]]
        pair = z_ref[i, :, 1024:1152]
        rots += [pair, jnp.concatenate([pair[:, 64:], pair[:, :64]], axis=1)]
    lat = jnp.concatenate(lats, axis=0)
    rot = jnp.concatenate(rots, axis=0)
    absorbed = a0_ref[...] + a1_ref[...]
    scores = lax.dot_general(absorbed, lat, LAST, preferred_element_type=F32)
    scores = scores + lax.dot_general(t_ref[...], rot, LAST, preferred_element_type=F32)
    scores = scores * ((PLAIN_MATCH_SPAN + QK_ROPE) ** (-0.5))
    top = jnp.max(scores, axis=-1, keepdims=True).astype(BF16).astype(F32)
    weight = jnp.exp(scores - top)
    total = jnp.sum(weight, axis=-1, keepdims=True)
    context = jnp.dot(weight.astype(BF16), lat, preferred_element_type=F32)
    high = total.astype(BF16).astype(F32)
    low = total - high
    top = jnp.broadcast_to(top, context.shape)
    high = jnp.broadcast_to(high, context.shape)
    low = jnp.broadcast_to(low, context.shape)
    lat_t = lat.T
    rot_t = rot.astype(F32).T
    for t in range(out_ref.shape[0]):
        slot = out_ref.shape[0] - 1 - t
        out_ref[slot, 0:64, :] = lat_t[64 * t : 64 * (t + 1)]
        mine = slice(2 * t, 2 * t + 2)
        block = jnp.concatenate(
            [rot_t[8 * t : 8 * t + 8], context[mine], top[mine], high[mine], low[mine]], axis=0
        )
        out_ref[slot, 64:80, :] = block.astype(BF16)


def order_payload_kernel(p0_ref, p1_ref, p2_ref, p3_ref, out_ref):
    x, core = lax.axis_index("x"), lax.axis_index("c")
    for d, piece in enumerate((p0_ref, p1_ref, p2_ref, p3_ref)):
        chip = (x + 4 - d) % 4
        out_ref[2 * chip + core] = piece[0]
        out_ref[2 * chip + 1 - core] = piece[1]


def finish_kernel(y_ref, w_ref, st_ref, rt_ref, fr_ref):
    count = y_ref.shape[0]
    for q in range(4):
        for o in range(4):
            for j in range(2):
                lanes = slice((4 * q + o) * 32, (4 * q + o) * 32 + 32)
                tile = jnp.concatenate(
                    [y_ref[count - 1 - (4 * j + k), 0:80, lanes] for k in range(4)], axis=1
                )
                at = (4 * q + o) * 256 + j * 128
                st_ref[:, at : at + 128] = tile[0:64]
                rt_ref[:, at : at + 128] = tile[64:72]
    tails = [y_ref[t, 64:80, :].astype(F32)[8:16] for t in range(count)]
    tops = [v[2:4] for v in tails]
    peak = tops[0]
    for v in tops[1:]:
        peak = jnp.maximum(peak, v)
    number = jnp.zeros_like(peak)
    denominator = jnp.zeros_like(peak)
    for v, top in zip(tails, tops):
        scale = jnp.exp(top - peak)
        number = number + scale * v[0:2]
        denominator = denominator + scale * (v[4:6] + v[6:8])
    context = (number / denominator).astype(BF16)
    weight = w_ref[...].reshape(count * 64, 256)
    values = jnp.dot(context, weight, preferred_element_type=F32)
    values = jnp.concatenate([values[0:1, 0:128], values[1:2, 128:256]], axis=0)
    mean = jnp.mean(values * values, axis=-1, keepdims=True)
    fr_ref[...] = (values * lax.rsqrt(mean + norm_eps)).astype(BF16)


def exchange(array, sp, tp, over_sp):
    if over_sp:
        groups = [[s * tp + t for s in reversed(range(sp))] for t in range(tp)]
    else:
        groups = [[s * tp + t for t in reversed(range(tp))] for s in range(sp)]
    return lax.all_to_all(array, SP_TP, 0, 0, tiled=True, axis_index_groups=groups)


def call(kernel, out_shape, flops, moved, **kwargs):
    return pl.pallas_call(
        kernel,
        out_shape=out_shape,
        **kwargs,
        cost_estimate=pl.CostEstimate(flops=flops, bytes_accessed=moved, transcendentals=0),
        compiler_params=pltpu.CompilerParams(vmem_limit_bytes=32 * 1024 * 1024),
    )


def shards(
    layer_input,
    input_gain,
    narrowing_matrix,
    rotary_down,
    summary_scaling,
    lookup_widening,
    payload_widening,
    query_nope,
    query_rotary,
):
    seqs, pos_local, width = layer_input.shape
    tp = lax.axis_size(TP)
    sp = lax.axis_size("sp")
    shape = jax.ShapeDtypeStruct

    at = (lax.axis_index("x"), lax.axis_index("c"))
    swap = [(0, 1), (1, 0)]
    lookup_other = lax.ppermute(lookup_widening, "c", swap)
    payload_other = lax.ppermute(payload_widening, "c", swap)
    nope_other = lax.ppermute(query_nope[0], "c", swap)
    rotary_other = lax.ppermute(query_rotary[0], "c", swap)
    table = call(
        table_kernel,
        shape((2, pos_local, QK_ROPE), F32),
        30_000_000_000,
        60_000_000,
    )(jnp.tile(frequencies(), 2)[None])
    query = call(
        place_queries_kernel,
        shape((2 * tp, 256), BF16),
        1_000_000,
        10_000,
    )(query_nope[0], query_rotary[0], nope_other, rotary_other)
    near, far = [(0, 1), (1, 0), (2, 3), (3, 2)], [(0, 3), (3, 0), (1, 2), (2, 1)]
    moved = lax.ppermute(query, "x", far)
    query = query + moved
    moved = lax.ppermute(query, "x", near)

    sent = call(
        project_kernel,
        shape((seqs, pos_local // 2, 1152), BF16),
        1_300_000_000,
        5_000_000,
    )(
        layer_input.reshape(seqs * pos_local, width),
        input_gain[None],
        narrowing_matrix,
        rotary_down.T,
        summary_scaling[None],
        table,
    )
    held = exchange(sent, sp, tp, True)

    query = query + moved
    turn = query[:, 128 : 128 + QK_ROPE]
    query = query[:, :128]
    own, partner = (
        jnp.einsum("hd,chd->hc", query, weight, preferred_element_type=F32).astype(BF16)
        for weight in (lookup_widening, lookup_other)
    )
    first, second = jnp.where(at[1] == 0, own, partner), jnp.where(at[1] == 0, partner, own)
    share = jnp.concatenate([first, second] * 4, axis=1)
    lane = lax.broadcasted_iota(jnp.int32, (2 * tp, 512), 1) // 128
    placed = jnp.where(lane == at[0], share, jnp.zeros((), BF16))
    moved = lax.ppermute(placed, "x", near)
    placed = placed + moved
    other = lax.ppermute(placed, "x", far)
    each = payload_widening.shape[0]
    parts = call(
        pack_payload_kernel,
        [shape((2, each, 256), BF16)] * 4,
        1_000_000,
        1_000_000,
        scratch_shapes=[pltpu.VMEM((each * 2 * tp, 128), F32)] * 2,
    )(payload_widening, payload_other)
    pieces = [parts[0]]
    for d in (1, 2, 3):
        pieces.append(lax.ppermute(parts[d], "x", [(i, (i + d) % 4) for i in range(4)]))
    turned = rotate(turn.astype(F32), F32(seqs * 0 + sp * tp * pos_local)).astype(BF16)
    turned = jnp.concatenate([turned, jnp.zeros_like(turned)], axis=1)

    piece = call(attend_kernel, shape((tp, 80, 512), BF16), 600_000_000, 1_300_000)(
        held, placed, other, turned
    )
    arrived = exchange(piece, sp, tp, False)
    weight = call(order_payload_kernel, shape((tp, each, 256), BF16), 1_000_000, 500_000)(*pieces)

    total = sp * tp * pos_local
    stored, rotary, first = call(
        finish_kernel,
        (shape((64, total), BF16), shape((8, total), BF16), shape((2, 128), BF16)),
        10_000_000,
        1_800_000,
    )(arrived, weight)
    return stored.T[None], rotary.T[None], first[None]


def solution(mesh):
    torus = Mesh(mesh.devices.reshape(mesh.shape["sp"], 4, 2), SP_TP)
    in_specs = (
        P(None, SP_TP, None),
        P(),
        P(),
        P(),
        P(),
        P(TP, None, None),
        P(TP, None, None),
        P("sp", TP, None),
        P("sp", TP, None),
    )
    out_specs = (P("sp", None, TP), P("sp", None, TP), P("sp", TP, None))

    return jax.shard_map(
        shards, mesh=torus, in_specs=in_specs, out_specs=out_specs, check_vma=False
    )
```

```python
import jax
import jax.numpy as jnp
from jax import lax
from jax.experimental import pallas as pl
from jax.experimental.pallas import tpu as pltpu
from jax.sharding import Mesh
from jax.sharding import PartitionSpec as P

QK_ROPE = 64
PLAIN_MATCH_SPAN = 128
TP = ("x", "c")
SP_TP = ("sp", "x", "c")

norm_eps = 1e-06
rotary_base = 10000.0
F32 = jnp.float32
BF16 = jnp.bfloat16
LAST = (((1,), (1,)), ((), ()))


def frequencies():
    half = QK_ROPE // 2
    return 1.0 / rotary_base ** (jnp.arange(half, dtype=F32) * 2.0 / QK_ROPE)


def rotate(vector, position):
    half_width = vector.shape[-1] // 2
    angles = position * frequencies()
    first_half = vector[..., :half_width]
    second_half = vector[..., half_width:]
    return jnp.concatenate(
        [
            first_half * jnp.cos(angles) - second_half * jnp.sin(angles),
            second_half * jnp.cos(angles) + first_half * jnp.sin(angles),
        ],
        axis=-1,
    )


def table_kernel(freq_ref, out_ref):
    rows, lanes = out_ref.shape[1:]
    first = lax.axis_index(SP_TP) * rows
    position = first + lax.broadcasted_iota(jnp.int32, (rows, lanes), 0)
    angles = position.astype(F32) * freq_ref[...]
    lane = lax.broadcasted_iota(jnp.int32, (rows, lanes), 1)
    sin = jnp.sin(angles)
    out_ref[0] = jnp.cos(angles)
    out_ref[1] = jnp.where(lane < lanes // 2, -sin, sin)


def place_queries_kernel(qn_ref, qr_ref, qn_other_ref, qr_other_ref, out_ref):
    blank = jnp.zeros(qr_ref.shape, F32)
    mine = jnp.concatenate([qn_ref[...].astype(F32), qr_ref[...].astype(F32), blank], axis=1)
    partner = jnp.concatenate(
        [qn_other_ref[...].astype(F32), qr_other_ref[...].astype(F32), blank], axis=1
    )
    core = lax.axis_index("c")
    first = jnp.where(core == 0, mine, partner)
    second = jnp.where(core == 0, partner, mine)
    rows = jnp.concatenate([first, second] * 4, axis=0)
    row = lax.broadcasted_iota(jnp.int32, rows.shape, 0) // 4
    out_ref[...] = jnp.where(row == lax.axis_index("x"), rows, 0.0).astype(BF16)


def pack_payload_kernel(share_ref, own_ref, other_ref, *refs):
    x, core = lax.axis_index("x"), lax.axis_index("c")
    outs, (own_f32, other_f32) = refs[:4], refs[4:]
    each = own_ref.shape[0]
    absorbed = jnp.concatenate([share_ref[...], jnp.zeros_like(share_ref)], axis=1)
    heads = own_ref.shape[1]
    own_f32[...] = own_ref[...].astype(F32).reshape(own_f32.shape)
    other_f32[...] = other_ref[...].astype(F32).reshape(other_f32.shape)
    for d, out_ref in enumerate(outs):
        first = 2 * (2 * ((x + d) % 4) + core)
        for r, source in enumerate((own_f32, other_f32)):
            for h in range(2):
                rows = source[pl.ds(first + h, each, stride=heads), :]
                out_ref[r, 0:each, h * 128 : (h + 1) * 128] = rows.astype(BF16)
            out_ref[r, each:, :] = absorbed


def project_kernel(x_ref, gain_ref, w_ref, r_ref, scal_ref, cs_ref, out_ref):
    count = out_ref.shape[0]
    x = x_ref[...].astype(F32)
    scale = lax.rsqrt(jnp.mean(x * x, axis=-1, keepdims=True) + norm_eps)
    gained = (x * gain_ref[...]).astype(BF16)
    lat = jnp.dot(gained, w_ref[...], preferred_element_type=F32)
    rot = lax.dot_general(gained, r_ref[...], LAST, preferred_element_type=F32)
    lat = (lat * scale).astype(BF16).astype(F32)
    rot = (rot * scale).astype(BF16).astype(F32)
    mean = jnp.mean(lat * lat, axis=-1, keepdims=True)
    lat = (lat * lax.rsqrt(mean + norm_eps) * scal_ref[...]).astype(BF16)
    cos = jnp.concatenate([cs_ref[0]] * count, axis=0)
    sin = jnp.concatenate([cs_ref[1]] * count, axis=0)
    swapped = jnp.concatenate([rot[:, 32:], rot[:, :32]], axis=1)
    rot = rot * cos + swapped * sin
    for s in range(count):
        slot = count - 1 - s
        at = s * 32
        pair = jnp.concatenate([rot[at : at + 16], rot[at + 16 : at + 32]], axis=1)
        out_ref[slot, :, 0:512] = lat[at : at + 16]
        out_ref[slot, :, 512:1024] = lat[at + 16 : at + 32]
        out_ref[slot, :, 1024:1152] = pair.astype(BF16)


def attend_kernel(z_ref, p0_ref, p1_ref, p2_ref, p3_ref, t_ref, out_ref, w_ref, a_ref):
    core = lax.axis_index("c")
    for d, piece in enumerate((p0_ref, p1_ref, p2_ref, p3_ref)):
        chip = (lax.axis_index("x") + 4 - d) % 4
        a_ref[:, pl.ds(pl.multiple_of(chip * 128, 128), 128)] = piece[0, 64:80, 0:128]
        w_ref[2 * chip + core] = piece[0, 0:64]
        w_ref[2 * chip + 1 - core] = piece[1, 0:64]
    lats, rots = [], []
    for i in range(z_ref.shape[0] - 1, -1, -1):
        lats += [z_ref[i, :, 0:512], z_ref[i, :, 512:1024]]
        pair = z_ref[i, :, 1024:1152]
        rots += [pair, jnp.concatenate([pair[:, 64:], pair[:, :64]], axis=1)]
    lat = jnp.concatenate(lats, axis=0)
    rot = jnp.concatenate(rots, axis=0)
    absorbed = a_ref[...]
    scores = lax.dot_general(absorbed, lat, LAST, preferred_element_type=F32)
    scores = scores + lax.dot_general(t_ref[...], rot, LAST, preferred_element_type=F32)
    scores = scores * ((PLAIN_MATCH_SPAN + QK_ROPE) ** (-0.5))
    top = jnp.max(scores, axis=-1, keepdims=True).astype(BF16).astype(F32)
    weight = jnp.exp(scores - top)
    total = jnp.sum(weight, axis=-1, keepdims=True)
    context = jnp.dot(weight.astype(BF16), lat, preferred_element_type=F32)
    high = total.astype(BF16).astype(F32)
    low = total - high
    top = jnp.broadcast_to(top, context.shape)
    high = jnp.broadcast_to(high, context.shape)
    low = jnp.broadcast_to(low, context.shape)
    lat_t = lat.T
    rot_t = rot.astype(F32).T
    for t in range(out_ref.shape[0]):
        slot = out_ref.shape[0] - 1 - t
        out_ref[slot, 0:64, :] = lat_t[64 * t : 64 * (t + 1)]
        mine = slice(2 * t, 2 * t + 2)
        block = jnp.concatenate(
            [rot_t[8 * t : 8 * t + 8], context[mine], top[mine], high[mine], low[mine]], axis=0
        )
        out_ref[slot, 64:80, :] = block.astype(BF16)


def finish_kernel(y_ref, w_ref, st_ref, rt_ref, fr_ref):
    count = y_ref.shape[0]
    for q in range(4):
        for o in range(4):
            for j in range(2):
                lanes = slice((4 * q + o) * 32, (4 * q + o) * 32 + 32)
                tile = jnp.concatenate(
                    [y_ref[count - 1 - (4 * j + k), 0:80, lanes] for k in range(4)], axis=1
                )
                at = (4 * q + o) * 256 + j * 128
                st_ref[:, at : at + 128] = tile[0:64]
                rt_ref[:, at : at + 128] = tile[64:72]
    tails = [y_ref[t, 64:80, :].astype(F32)[8:16] for t in range(count)]
    tops = [v[2:4] for v in tails]
    peak = tops[0]
    for v in tops[1:]:
        peak = jnp.maximum(peak, v)
    number = jnp.zeros_like(peak)
    denominator = jnp.zeros_like(peak)
    for v, top in zip(tails, tops):
        scale = jnp.exp(top - peak)
        number = number + scale * v[0:2]
        denominator = denominator + scale * (v[4:6] + v[6:8])
    context = (number / denominator).astype(BF16)
    weight = w_ref[...].reshape(count * 64, 256)
    values = jnp.dot(context, weight, preferred_element_type=F32)
    values = jnp.concatenate([values[0:1, 0:128], values[1:2, 128:256]], axis=0)
    mean = jnp.mean(values * values, axis=-1, keepdims=True)
    fr_ref[...] = (values * lax.rsqrt(mean + norm_eps)).astype(BF16)


def exchange(array, sp, tp, over_sp):
    if over_sp:
        groups = [[s * tp + t for s in reversed(range(sp))] for t in range(tp)]
    else:
        groups = [[s * tp + t for t in reversed(range(tp))] for s in range(sp)]
    return lax.all_to_all(array, SP_TP, 0, 0, tiled=True, axis_index_groups=groups)


def call(kernel, out_shape, flops, moved, **kwargs):
    return pl.pallas_call(
        kernel,
        out_shape=out_shape,
        **kwargs,
        cost_estimate=pl.CostEstimate(flops=flops, bytes_accessed=moved, transcendentals=0),
        compiler_params=pltpu.CompilerParams(vmem_limit_bytes=32 * 1024 * 1024),
    )


def shards(
    layer_input,
    input_gain,
    narrowing_matrix,
    rotary_down,
    summary_scaling,
    lookup_widening,
    payload_widening,
    query_nope,
    query_rotary,
):
    seqs, pos_local, width = layer_input.shape
    tp = lax.axis_size(TP)
    sp = lax.axis_size("sp")
    shape = jax.ShapeDtypeStruct

    at = (lax.axis_index("x"), lax.axis_index("c"))
    swap = [(0, 1), (1, 0)]
    lookup_other = lax.ppermute(lookup_widening, "c", swap)
    payload_other = lax.ppermute(payload_widening, "c", swap)
    nope_other = lax.ppermute(query_nope[0], "c", swap)
    rotary_other = lax.ppermute(query_rotary[0], "c", swap)
    table = call(
        table_kernel,
        shape((2, pos_local, QK_ROPE), F32),
        30_000_000_000,
        60_000_000,
    )(jnp.tile(frequencies(), 2)[None])
    query = call(
        place_queries_kernel,
        shape((2 * tp, 256), BF16),
        1_000_000,
        10_000,
    )(query_nope[0], query_rotary[0], nope_other, rotary_other)
    near, far = [(0, 1), (1, 0), (2, 3), (3, 2)], [(0, 3), (3, 0), (1, 2), (2, 1)]
    moved = lax.ppermute(query, "x", far)
    query = query + moved
    moved = lax.ppermute(query, "x", near)

    sent = call(
        project_kernel,
        shape((seqs, pos_local // 2, 1152), BF16),
        1_300_000_000,
        5_000_000,
    )(
        layer_input.reshape(seqs * pos_local, width),
        input_gain[None],
        narrowing_matrix,
        rotary_down.T,
        summary_scaling[None],
        table,
    )
    held = exchange(sent, sp, tp, True)

    query = query + moved
    turn = query[:, 128 : 128 + QK_ROPE]
    query = query[:, :128]
    own, partner = (
        jnp.einsum("hd,chd->hc", query, weight, preferred_element_type=F32).astype(BF16)
        for weight in (lookup_widening, lookup_other)
    )
    first, second = jnp.where(at[1] == 0, own, partner), jnp.where(at[1] == 0, partner, own)
    share = jnp.concatenate([first, second], axis=1)
    each = payload_widening.shape[0]
    parts = call(
        pack_payload_kernel,
        [shape((2, each + 2 * tp, 256), BF16)] * 4,
        1_000_000,
        1_000_000,
        scratch_shapes=[pltpu.VMEM((each * 2 * tp, 128), F32)] * 2,
    )(share, payload_widening, payload_other)
    pieces = [parts[0]]
    for d in (1, 2, 3):
        pieces.append(lax.ppermute(parts[d], "x", [(i, (i + d) % 4) for i in range(4)]))
    turned = rotate(turn.astype(F32), F32(seqs * 0 + sp * tp * pos_local)).astype(BF16)
    turned = jnp.concatenate([turned, jnp.zeros_like(turned)], axis=1)

    piece, weight = call(
        attend_kernel,
        (shape((tp, 80, 512), BF16), shape((tp, each, 256), BF16)),
        600_000_000,
        1_300_000,
        scratch_shapes=[pltpu.VMEM((2 * tp, 512), BF16)],
    )(held, *pieces, turned)
    arrived = exchange(piece, sp, tp, False)
    total = sp * tp * pos_local
    stored, rotary, first = call(
        finish_kernel,
        (shape((64, total), BF16), shape((8, total), BF16), shape((2, 128), BF16)),
        10_000_000,
        1_800_000,
    )(arrived, weight)
    return stored.T[None], rotary.T[None], first[None]


def solution(mesh):
    torus = Mesh(mesh.devices.reshape(mesh.shape["sp"], 4, 2), SP_TP)
    in_specs = (
        P(None, SP_TP, None),
        P(),
        P(),
        P(),
        P(),
        P(TP, None, None),
        P(TP, None, None),
        P("sp", TP, None),
        P("sp", TP, None),
    )
    out_specs = (P("sp", None, TP), P("sp", None, TP), P("sp", TP, None))

    return jax.shard_map(
        shards, mesh=torus, in_specs=in_specs, out_specs=out_specs, check_vma=False
    )
```

```python
import jax
import jax.numpy as jnp
from jax import lax
from jax.experimental import pallas as pl
from jax.experimental.pallas import tpu as pltpu
from jax.sharding import Mesh
from jax.sharding import PartitionSpec as P

QK_ROPE = 64
PLAIN_MATCH_SPAN = 128
TP = ("x", "c")
SP_TP = ("sp", "x", "c")

norm_eps = 1e-06
rotary_base = 10000.0
F32 = jnp.float32
BF16 = jnp.bfloat16
LAST = (((1,), (1,)), ((), ()))


def frequencies():
    half = QK_ROPE // 2
    return 1.0 / rotary_base ** (jnp.arange(half, dtype=F32) * 2.0 / QK_ROPE)


def rotate(vector, position):
    half_width = vector.shape[-1] // 2
    angles = position * frequencies()
    first_half = vector[..., :half_width]
    second_half = vector[..., half_width:]
    return jnp.concatenate(
        [
            first_half * jnp.cos(angles) - second_half * jnp.sin(angles),
            second_half * jnp.cos(angles) + first_half * jnp.sin(angles),
        ],
        axis=-1,
    )


def table_kernel(freq_ref, out_ref):
    rows, lanes = out_ref.shape[1:]
    first = lax.axis_index(SP_TP) * rows
    position = first + lax.broadcasted_iota(jnp.int32, (rows, lanes), 0)
    angles = position.astype(F32) * freq_ref[...]
    lane = lax.broadcasted_iota(jnp.int32, (rows, lanes), 1)
    sin = jnp.sin(angles)
    out_ref[0] = jnp.cos(angles)
    out_ref[1] = jnp.where(lane < lanes // 2, -sin, sin)


def place_queries_kernel(qn_ref, qr_ref, qn_other_ref, qr_other_ref, out_ref):
    blank = jnp.zeros(qr_ref.shape, F32)
    mine = jnp.concatenate([qn_ref[...].astype(F32), qr_ref[...].astype(F32), blank], axis=1)
    partner = jnp.concatenate(
        [qn_other_ref[...].astype(F32), qr_other_ref[...].astype(F32), blank], axis=1
    )
    core = lax.axis_index("c")
    first = jnp.where(core == 0, mine, partner)
    second = jnp.where(core == 0, partner, mine)
    rows = jnp.concatenate([first, second] * 4, axis=0)
    row = lax.broadcasted_iota(jnp.int32, rows.shape, 0) // 4
    out_ref[...] = jnp.where(row == lax.axis_index("x"), rows, 0.0).astype(BF16)


def pack_payload_kernel(mine_ref, partner_ref, own_ref, other_ref, *refs):
    x, core = lax.axis_index("x"), lax.axis_index("c")
    outs, (own_f32, other_f32) = refs[:4], refs[4:]
    each = own_ref.shape[0]
    mine, partner = mine_ref[...], partner_ref[...]
    first, second = jnp.where(core == 0, mine, partner), jnp.where(core == 0, partner, mine)
    blank = jnp.zeros((mine.shape[0], 128), F32)
    absorbed = jnp.concatenate([first, second, blank], axis=1).astype(BF16)
    heads = own_ref.shape[1]
    own_f32[0 : each * heads, :] = own_ref[...].astype(F32).reshape(each * heads, 128)
    other_f32[0 : each * heads, :] = other_ref[...].astype(F32).reshape(each * heads, 128)
    for d, out_ref in enumerate(outs):
        first = 2 * (2 * ((x + d) % 4) + core)
        for r, source in enumerate((own_f32, other_f32)):
            for h in range(2):
                rows = source[pl.ds(first + h, each, stride=heads), :]
                out_ref[r, 0:each, h * 128 : (h + 1) * 128] = rows.astype(BF16)
            out_ref[r, each:, :] = absorbed


def project_kernel(x_ref, gain_ref, w_ref, r_ref, scal_ref, cs_ref, out_ref):
    count = out_ref.shape[0]
    x = x_ref[...].astype(F32)
    scale = lax.rsqrt(jnp.mean(x * x, axis=-1, keepdims=True) + norm_eps)
    gained = (x * gain_ref[...]).astype(BF16)
    rot = lax.dot_general(r_ref[...], gained, LAST, preferred_element_type=F32).T
    lat = jnp.dot(gained, w_ref[...], preferred_element_type=F32)
    lat = (lat * scale).astype(BF16).astype(F32)
    rot = (rot * scale).astype(BF16).astype(F32)
    mean = jnp.mean(lat * lat, axis=-1, keepdims=True)
    lat = (lat * lax.rsqrt(mean + norm_eps) * scal_ref[...]).astype(BF16)
    cos = jnp.concatenate([cs_ref[0]] * count, axis=0)
    sin = jnp.concatenate([cs_ref[1]] * count, axis=0)
    swapped = jnp.concatenate([rot[:, 32:], rot[:, :32]], axis=1)
    rot = rot * cos + swapped * sin
    for s in range(count):
        slot = count - 1 - s
        at = s * 32
        pair = jnp.concatenate([rot[at : at + 16], rot[at + 16 : at + 32]], axis=1)
        out_ref[slot, :, 0:512] = lat[at : at + 16]
        out_ref[slot, :, 512:1024] = lat[at + 16 : at + 32]
        out_ref[slot, :, 1024:1152] = pair.astype(BF16)


def attend_kernel(z_ref, p0_ref, p1_ref, p2_ref, p3_ref, t_ref, out_ref, w_ref, a_ref):
    core = lax.axis_index("c")
    for d, piece in enumerate((p0_ref, p1_ref, p2_ref, p3_ref)):
        chip = (lax.axis_index("x") + 4 - d) % 4
        a_ref[:, pl.ds(pl.multiple_of(chip * 128, 128), 128)] = piece[0, 64:80, 0:128]
        w_ref[2 * chip + core] = piece[0, 0:64]
        w_ref[2 * chip + 1 - core] = piece[1, 0:64]
    lats, rots = [], []
    for i in range(z_ref.shape[0] - 1, -1, -1):
        lats += [z_ref[i, :, 0:512], z_ref[i, :, 512:1024]]
        pair = z_ref[i, :, 1024:1152]
        rots += [pair, jnp.concatenate([pair[:, 64:], pair[:, :64]], axis=1)]
    lat = jnp.concatenate(lats, axis=0)
    rot = jnp.concatenate(rots, axis=0)
    absorbed = a_ref[...]
    scores = lax.dot_general(absorbed, lat, LAST, preferred_element_type=F32)
    scores = scores + lax.dot_general(t_ref[...], rot, LAST, preferred_element_type=F32)
    scores = scores * ((PLAIN_MATCH_SPAN + QK_ROPE) ** (-0.5))
    top = jnp.max(scores, axis=-1, keepdims=True).astype(BF16).astype(F32)
    weight = jnp.exp(scores - top)
    total = jnp.sum(weight, axis=-1, keepdims=True)
    context = jnp.dot(weight.astype(BF16), lat, preferred_element_type=F32)
    high = total.astype(BF16).astype(F32)
    low = total - high
    top = jnp.broadcast_to(top, context.shape)
    high = jnp.broadcast_to(high, context.shape)
    low = jnp.broadcast_to(low, context.shape)
    lat_t = lat.T
    rot_t = rot.astype(F32).T
    for t in range(out_ref.shape[0]):
        slot = out_ref.shape[0] - 1 - t
        out_ref[slot, 0:64, :] = lat_t[64 * t : 64 * (t + 1)]
        mine = slice(2 * t, 2 * t + 2)
        block = jnp.concatenate(
            [rot_t[8 * t : 8 * t + 8], context[mine], top[mine], high[mine], low[mine]], axis=0
        )
        out_ref[slot, 64:80, :] = block.astype(BF16)


def finish_kernel(y_ref, w_ref, st_ref, rt_ref, fr_ref):
    count = y_ref.shape[0]
    for q in range(4):
        for o in range(4):
            for j in range(2):
                lanes = slice((4 * q + o) * 32, (4 * q + o) * 32 + 32)
                tile = jnp.concatenate(
                    [y_ref[count - 1 - (4 * j + k), 0:80, lanes] for k in range(4)], axis=1
                )
                at = (4 * q + o) * 256 + j * 128
                st_ref[:, at : at + 128] = tile[0:64]
                rt_ref[:, at : at + 128] = tile[64:72]
    tails = [y_ref[t, 64:80, :].astype(F32)[8:16] for t in range(count)]
    tops = [v[2:4] for v in tails]
    peak = tops[0]
    for v in tops[1:]:
        peak = jnp.maximum(peak, v)
    number = jnp.zeros_like(peak)
    denominator = jnp.zeros_like(peak)
    for v, top in zip(tails, tops):
        scale = jnp.exp(top - peak)
        number = number + scale * v[0:2]
        denominator = denominator + scale * (v[4:6] + v[6:8])
    context = (number / denominator).astype(BF16)
    weight = w_ref[...].reshape(count * 64, 256)
    values = jnp.dot(context, weight, preferred_element_type=F32)
    values = jnp.concatenate([values[0:1, 0:128], values[1:2, 128:256]], axis=0)
    mean = jnp.mean(values * values, axis=-1, keepdims=True)
    fr_ref[...] = (values * lax.rsqrt(mean + norm_eps)).astype(BF16)


def exchange(array, sp, tp, over_sp):
    if over_sp:
        groups = [[s * tp + t for s in reversed(range(sp))] for t in range(tp)]
    else:
        groups = [[s * tp + t for t in reversed(range(tp))] for s in range(sp)]
    return lax.all_to_all(array, SP_TP, 0, 0, tiled=True, axis_index_groups=groups)


def call(kernel, out_shape, flops, moved, **kwargs):
    return pl.pallas_call(
        kernel,
        out_shape=out_shape,
        **kwargs,
        cost_estimate=pl.CostEstimate(flops=flops, bytes_accessed=moved, transcendentals=0),
        compiler_params=pltpu.CompilerParams(vmem_limit_bytes=32 * 1024 * 1024),
    )


def shards(
    layer_input,
    input_gain,
    narrowing_matrix,
    rotary_down,
    summary_scaling,
    lookup_widening,
    payload_widening,
    query_nope,
    query_rotary,
):
    seqs, pos_local, width = layer_input.shape
    tp = lax.axis_size(TP)
    sp = lax.axis_size("sp")
    shape = jax.ShapeDtypeStruct

    swap = [(0, 1), (1, 0)]
    lookup_other = lax.ppermute(lookup_widening, "c", swap)
    payload_other = lax.ppermute(payload_widening, "c", swap)
    nope_other = lax.ppermute(query_nope[0], "c", swap)
    rotary_other = lax.ppermute(query_rotary[0], "c", swap)
    table = call(
        table_kernel,
        shape((2, pos_local, QK_ROPE), F32),
        30_000_000_000,
        60_000_000,
    )(jnp.tile(frequencies(), 2)[None])
    query = call(
        place_queries_kernel,
        shape((2 * tp, 256), BF16),
        1_000_000,
        10_000,
    )(query_nope[0], query_rotary[0], nope_other, rotary_other)
    near, far = [(0, 1), (1, 0), (2, 3), (3, 2)], [(0, 3), (3, 0), (1, 2), (2, 1)]
    moved = lax.ppermute(query, "x", far)
    query = query + moved
    moved = lax.ppermute(query, "x", near)

    sent = call(
        project_kernel,
        shape((seqs, pos_local // 2, 1152), BF16),
        1_300_000_000,
        5_000_000,
    )(
        layer_input.reshape(seqs * pos_local, width),
        input_gain[None],
        narrowing_matrix,
        rotary_down.T,
        summary_scaling[None],
        table,
    )
    held = exchange(sent, sp, tp, True)

    query = query + moved
    turn = query[:, 128 : 128 + QK_ROPE]
    query = query[:, :128]
    mine, partner = (
        jnp.einsum("hd,chd->hc", query, weight, preferred_element_type=F32)
        for weight in (lookup_widening, lookup_other)
    )
    each = payload_widening.shape[0]
    parts = call(
        pack_payload_kernel,
        [shape((2, each + 2 * tp, 256), BF16)] * 4,
        1_000_000,
        1_000_000,
        scratch_shapes=[pltpu.VMEM(((each + 1) * 2 * tp, 128), F32)] * 2,
    )(mine, partner, payload_widening, payload_other)
    pieces = [parts[0]]
    for d in (1, 2, 3):
        pieces.append(lax.ppermute(parts[d], "x", [(i, (i + d) % 4) for i in range(4)]))
    turned = rotate(turn.astype(F32), F32(seqs * 0 + sp * tp * pos_local)).astype(BF16)
    turned = jnp.concatenate([turned, jnp.zeros_like(turned)], axis=1)

    piece, weight = call(
        attend_kernel,
        (shape((tp, 80, 512), BF16), shape((tp, each, 256), BF16)),
        600_000_000,
        1_300_000,
        scratch_shapes=[pltpu.VMEM((2 * tp, 512), BF16)],
    )(held, *pieces, turned)
    arrived = exchange(piece, sp, tp, False)
    total = sp * tp * pos_local
    stored, rotary, first = call(
        finish_kernel,
        (shape((64, total), BF16), shape((8, total), BF16), shape((2, 128), BF16)),
        10_000_000,
        1_800_000,
    )(arrived, weight)
    return stored.T[None], rotary.T[None], first[None]


def solution(mesh):
    torus = Mesh(mesh.devices.reshape(mesh.shape["sp"], 4, 2), SP_TP)
    in_specs = (
        P(None, SP_TP, None),
        P(),
        P(),
        P(),
        P(),
        P(TP, None, None),
        P(TP, None, None),
        P("sp", TP, None),
        P("sp", TP, None),
    )
    out_specs = (P("sp", None, TP), P("sp", None, TP), P("sp", TP, None))

    return jax.shard_map(
        shards, mesh=torus, in_specs=in_specs, out_specs=out_specs, check_vma=False
    )
```
